32 devices in a mesh: sp: 4 (over y, x), tp: 8 (over z, core).
Axes of the slice: x: 2, y: 2, z: 4, core: 2. Of those that a mesh axis runs over, the one named last changes fastest.
Arguments:
- query_heads: bfloat16 [4096, 2048], P('sp', 'tp'), may hold values from -256 to 256
- key_heads: bfloat16 [4096, 1024], P('sp', 'tp'), may hold values from -7 to 7
- value_heads: bfloat16 [4096, 1024], P('sp', 'tp'), may hold values from -6 to 6
- sink_logit: float32 [32], P('tp'), may hold values from 3 to 7
- residual: bfloat16 [4096, 2048], P(('sp', 'tp')), may hold values from -6 to 6
- out_weight: bfloat16 [2048, 2048], replicated, may hold values from -0.5 to 0.5
- norm_gain: float32 [2048], replicated, may hold values from 0.1 to 1.9
- routes: int32 [4096, 2], P('sp'), may hold values from 0 to 3, all different within a row; in each aligned block of 128 rows (0 to 127, 128 to 255, ...) at most 80 rows name the same one
- route_weight: float32 [4096, 2], P(('sp', 'tp')), may hold values from 0.2 to 1
- gate_weight: bfloat16 [4, 2048, 2048], P('sp', None, 'tp'), may hold values from -0.3125 to 0.3125
- up_weight: bfloat16 [4, 2048, 2048], P('sp', None, 'tp'), may hold values from -0.3125 to 0.3125
- down_weight: bfloat16 [4, 2048, 2048], P('sp', 'tp'), may hold values from -0.0625 to 0.0625
Outputs:
- updated: bfloat16 [4096, 2048], P(('sp', 'tp'))
The draws below stay inside these ranges and needn't reach their ends.
Inputs may be any that keep to these rules, and one draw needn't show every extreme that they name: `routes`: each row names 2 different experts. In each aligned block of 128 rows no expert is named more than 80 times, and in every draw some block names some expert exactly 80 times.
All inputs are finite; a program needn't handle non-finite values.
Results may differ from the reference program's by a relative error of at most 0.023.
Values may be sent and summed in bfloat16 or wider, within the bound.
No kernel may reach another device: no remote copies, remote signals or barrier semaphores. Data moves between devices by JAX's collectives and lax.ppermute only.
A program may use at most 128 MiB of HBM per device.

```python
import math
import jax
import jax.numpy as jnp
import numpy as np
from jax import lax

D = 2048
HEAD = 64
HQ = 32
KVH = 16
FF = 2048
WINDOW = 128
TOP = 2
SEQ = 4096
TOKENS = 4096
TOK_DEV = 128
EXPERTS = 4
CAP = 80
N_SP = 4
N_TP = 8


def drawn_keys(key):
    base = jnp.clip(jax.random.normal(jax.random.fold_in(key, 101), (SEQ, KVH * HEAD), jnp.float32), -6.0, 6.0)
    return base


def draw_key_heads(key, part):
    base = drawn_keys(key)
    return base.astype(jnp.bfloat16)


def draw_query_heads(key, part):
    queries = jnp.clip(jax.random.normal(jax.random.fold_in(key, 104), (SEQ, HQ * HEAD), jnp.float32), -6.0, 6.0)
    return queries.astype(jnp.bfloat16)


def steps_of(key, extent, shards, least, top_value):
    factor_of, own = 1.0, jax.random.fold_in(key, 6)
    for axis_at, blocks in shards:
        draws = jnp.exp(jax.random.uniform(jax.random.fold_in(own, axis_at), (blocks,), jnp.float32, least / len(shards), top_value / len(shards)))
        factor_of = factor_of * jnp.repeat(draws, extent[axis_at] // blocks).reshape([-1 if axis == axis_at else 1 for axis in range(len(extent))])
    return factor_of


def routed_block(stream_key, own, number, rows, amount, top, limit, slope):
    order = jax.random.permutation(stream_key, amount)
    packed, common = shares(amount, rows * top, limit, slope, True), shares(amount, rows * top, limit, slope, False)
    places = jnp.arange(amount)

    def named(lengths, offset_by):
        used = int((lengths > 0).sum())
        fixed = max(1, used // 4)
        shifted = fixed + (places - fixed + offset_by * (used - fixed)) % max(1, amount - fixed)
        return jnp.zeros((amount,), jnp.int32).at[order[jnp.where(places < fixed, places, shifted)]].set(jnp.asarray(lengths, jnp.int32))

    lengths = jnp.where(number % 4 == 0, named(packed, number // 4), named(common, number - number // 4 - 1))
    mixed = jax.random.permutation(jax.random.fold_in(own, 3), amount)
    donor, sink = mixed[0:amount // 2 * 2:2], mixed[1:amount // 2 * 2:2]
    room = jnp.minimum(lengths[donor] - 1, limit - lengths[sink]) // 2
    room = jnp.where((donor == order[0]) | (sink == order[0]) | (lengths[sink] == 0), 0, jnp.maximum(room, 0))
    shifted = jax.random.randint(jax.random.fold_in(own, 4), (amount // 2,), 0, 1 << 20) % (room + 1)
    lengths = lengths.at[donor].add(-shifted).at[sink].add(shifted)
    members = jnp.searchsorted(jnp.cumsum(lengths), jnp.arange(rows * top), side="right").astype(jnp.int32)
    grid = members.reshape(top, rows).T
    grid = grid[jax.random.permutation(jax.random.fold_in(own, 1), rows)]
    offset_by = jax.random.randint(jax.random.fold_in(own, 2), (rows, 1), 0, top)
    return jnp.take_along_axis(grid, (jnp.arange(top)[None, :] + offset_by) % top, axis=1)


def shares(amount, total, bound, slope, full):
    weights = [(1 << 20) // math.isqrt(standing ** slope) + 1 for standing in range(1, amount + 1)]
    largest = bound if full else min(bound, max(-(-total // amount), total * weights[0] // sum(weights)))
    least = 1 if total - largest >= amount - 1 else 0
    given, rest = [largest] + [least] * (amount - 1), total - largest - least * (amount - 1)
    while rest > 0:
        free = [i for i in range(1, amount) if given[i] < largest] or [i for i in range(1, amount) if given[i] < bound]
        pool, remaining = sum([weights[i] for i in free]), rest
        for i in free:
            extra = min(bound - given[i], max(1, remaining * weights[i] // pool), rest)
            given[i] = given[i] + extra
            rest = rest - extra
    return np.array(given)


def centred(own_key, dims, spread, limit, shards=(), held_as=jnp.bfloat16):
    array = spread * jax.random.normal(own_key, dims, jnp.float32)
    if shards:
        array = array * steps_of(own_key, dims, shards, -0.22, 0.18)
    return jnp.clip(array, -limit, limit).astype(held_as)


def setup_inputs(seed: int = 0) -> dict:
    arg_keys = jax.random.split(jax.random.key(seed), 13)
    query_heads = draw_query_heads(jax.random.fold_in(arg_keys[12], 71), 0)
    key_heads = draw_key_heads(jax.random.fold_in(arg_keys[12], 71), 0)
    value_heads = centred(arg_keys[2], (SEQ, KVH * HEAD), 1.0, 6.0, ((0, 4), (1, 8)))
    sink_logit = jnp.clip(3.0 + 4.0 * jax.random.uniform(arg_keys[3], (HQ,), jnp.float32) ** steps_of(arg_keys[3], (HQ,), ((0, 8),), -0.2, 0.2), 3.0, 7.0)
    residual = centred(arg_keys[4], (TOKENS, D), 1.0, 6.0, ((0, 32),))
    out_weight = centred(arg_keys[5], (HQ * HEAD, D), (HQ * HEAD // 16) ** -0.5, 0.5)
    norm_gain = jnp.clip(1.0 + 0.18 * jax.random.normal(arg_keys[6], (D,), jnp.float32), 0.1, 1.9)
    routes_keys = jax.random.split(jax.random.fold_in(arg_keys[7], 1), TOKENS // TOK_DEV)
    routes_turns = jax.random.permutation(jax.random.fold_in(arg_keys[7], 3), TOKENS // TOK_DEV)
    routes = jax.vmap(lambda own, number: routed_block(jax.random.fold_in(arg_keys[7], 2), own, number, TOK_DEV, EXPERTS, TOP, CAP, 1))(routes_keys, routes_turns).reshape((TOKENS, TOP))
    route_weight = jnp.clip(0.2 + 0.8 * jax.random.uniform(arg_keys[8], (TOKENS, TOP), jnp.float32) ** steps_of(arg_keys[8], (TOKENS, TOP), ((0, 32),), -0.2, 0.2), 0.2, 1.0)
    gate_weight = centred(arg_keys[9], (EXPERTS, D, FF), (D // 6) ** -0.5, 0.3125, ((0, 4), (2, 8)))
    up_weight = centred(arg_keys[10], (EXPERTS, D, FF), (D // 6) ** -0.5, 0.3125, ((0, 4), (2, 8)))
    down_weight = centred(arg_keys[11], (EXPERTS, FF, D), (FF * 4) ** -0.5, 0.0625, ((0, 4), (1, 8)))
    return {"query_heads": query_heads, "key_heads": key_heads, "value_heads": value_heads, "sink_logit": sink_logit, "residual": residual, "out_weight": out_weight, "norm_gain": norm_gain, "routes": routes, "route_weight": route_weight, "gate_weight": gate_weight, "up_weight": up_weight, "down_weight": down_weight}


eps = 1e-06
clamp_limit = 7.0
sigmoid_alpha = 1.702

def attention(query_heads, key_heads, value_heads, sink_logit):
    block_count = TOKENS // WINDOW
    group_size = HQ // KVH
    queries = query_heads.reshape(block_count, WINDOW, KVH, group_size, HEAD).transpose(2, 0, 1, 3, 4)
    key_blocks = key_heads.reshape(block_count, WINDOW, KVH, HEAD).transpose(2, 0, 1, 3)
    value_blocks = value_heads.reshape(block_count, WINDOW, KVH, HEAD).transpose(2, 0, 1, 3)
    sinks = sink_logit.reshape(KVH, group_size)
    query_pos = jnp.arange(WINDOW)[:, None]
    key_col = jnp.arange(2 * WINDOW)[None, :]
    distance = query_pos + WINDOW - key_col
    block_ids = jnp.arange(block_count)[:, None, None]
    key_global = (block_ids - 1) * WINDOW + key_col[None]
    allowed = (distance[None] >= 0) & (distance[None] < WINDOW) & (key_global >= 0)

    def banded(current):
        earlier = jnp.concatenate([jnp.zeros_like(current[:1]), current[:-1]], axis=0)
        return jnp.concatenate([earlier, current], axis=1)

    def one_head(items):
        query_part, key_part, value_part, sink_part = items
        key_band = banded(key_part).astype(jnp.float32)
        value_band = banded(value_part).astype(jnp.float32)
        scores = jnp.einsum('nqgd,nkd->ngqk', query_part.astype(jnp.float32), key_band) * HEAD ** (-0.5)
        logits = jnp.where(allowed[:, None], scores, -jnp.inf)
        sink_term = sink_part[None, :, None, None]
        row_max = jnp.maximum(lax.optimization_barrier(jnp.max(logits, axis=-1, keepdims=True)), sink_term)
        raised = jnp.exp(logits - row_max)
        weights_bf = (raised / (lax.optimization_barrier(jnp.sum(raised, axis=-1, keepdims=True)) + jnp.exp(sink_term - row_max))).astype(jnp.bfloat16)
        result = jnp.einsum('ngqk,nkd->nqgd', weights_bf.astype(jnp.float32), value_band)
        return result.astype(jnp.bfloat16)
    heads_out = lax.map(one_head, (queries, key_blocks, value_blocks, sinks))
    return heads_out.transpose(1, 2, 0, 3, 4).reshape(TOKENS, HQ * HEAD)

def reference(query_heads, key_heads, value_heads, sink_logit, residual, out_weight, norm_gain, routes, route_weight, gate_weight, up_weight, down_weight):
    attended = attention(query_heads, key_heads, value_heads, sink_logit)
    mixed = jnp.dot(attended, out_weight, preferred_element_type=jnp.float32)
    stream = (residual.astype(jnp.float32) + mixed).astype(jnp.bfloat16)
    stream32 = stream.astype(jnp.float32)
    normed = (stream32 * lax.rsqrt(lax.optimization_barrier(jnp.mean(stream32 * stream32, axis=-1, keepdims=True)) + eps) * norm_gain).astype(jnp.bfloat16)
    device_count = N_SP * N_TP
    choice_rows = routes.reshape(device_count, TOK_DEV * TOP)
    one_hot = (choice_rows[:, :, None] == jnp.arange(EXPERTS, dtype=jnp.int32)[None, None, :]).astype(jnp.int32)
    ranked = lax.optimization_barrier(jnp.sum((jnp.cumsum(one_hot, axis=1) - one_hot) * one_hot, axis=-1)).astype(jnp.int32)
    device_ids = jnp.arange(device_count, dtype=jnp.int32)[:, None]
    token_ids = device_ids * TOK_DEV + jnp.arange(TOK_DEV * TOP, dtype=jnp.int32)[None, :] // TOP
    table = jnp.full((device_count, EXPERTS, CAP), TOKENS, dtype=jnp.int32)
    table = table.at[device_ids, choice_rows, ranked].set(token_ids.astype(jnp.int32))
    padded = jnp.concatenate([normed, jnp.zeros((1, D), jnp.bfloat16)], axis=0)

    def run_expert(index):
        row_block = padded[table[:, index, :].reshape(-1)]
        gate_pre = jnp.dot(row_block, gate_weight[index], preferred_element_type=jnp.float32)
        upward = jnp.dot(row_block, up_weight[index], preferred_element_type=jnp.float32)
        capped = jnp.minimum(gate_pre, clamp_limit)
        linear = jnp.clip(upward, -clamp_limit, clamp_limit)
        hidden = (capped * jax.nn.sigmoid(sigmoid_alpha * capped) * (linear + 1.0)).astype(jnp.bfloat16)
        pieces = hidden.astype(jnp.float32).reshape(device_count * CAP, N_TP, FF // N_TP)
        down_pieces = down_weight[index].astype(jnp.float32).reshape(N_TP, FF // N_TP, D)
        partial_value = jnp.einsum('rjf,jfd->jrd', pieces, down_pieces).astype(jnp.bfloat16)
        return lax.optimization_barrier(jnp.sum(partial_value.astype(jnp.float32), axis=0)).astype(jnp.bfloat16)
    outputs = lax.map(run_expert, jnp.arange(EXPERTS, dtype=jnp.int32))
    shaped = outputs.reshape(EXPERTS, device_count, CAP, D)
    picked = shaped[choice_rows, device_ids, ranked]
    combined = lax.optimization_barrier(jnp.sum(picked.astype(jnp.float32).reshape(TOKENS, TOP, D) * route_weight[:, :, None], axis=1))
    return (stream32 + combined).astype(jnp.bfloat16)
```

```python
import functools

import jax
import jax.numpy as jnp
from jax import lax
from jax.experimental import pallas as pl
from jax.experimental.pallas import tpu as pltpu
from jax.sharding import PartitionSpec as P


HEAD = 64
WINDOW = 128
LANES = 128
SLOT_TILE = 16


eps = 1e-06
clamp_limit = 7.0
sigmoid_alpha = 1.702

F32 = jnp.float32
BF16 = jnp.bfloat16


def exchange(block, axis, partner):
    devices = range(lax.axis_size(axis))
    return lax.ppermute(block, axis, [(i, partner(i)) for i in devices])


def from_behind(block, axis):
    devices = range(lax.axis_size(axis))
    return lax.ppermute(block, axis, [(i - 1, i) for i in devices if i > 0])


def attention_kernel(
    info_ref, sink_ref, q_ref, k_ref, kp_ref, v_ref, vp_ref, tail_ref, out_ref, *, kv_local, group_size
):
    block = pl.program_id(0)
    head_block = block == 0
    kv_cols = kv_local * HEAD
    tail = tail_ref[...]
    k_prev = jnp.where(head_block, tail[:, :kv_cols], kp_ref[...])
    v_prev = jnp.where(head_block, tail[:, kv_cols:], vp_ref[...])
    k_now = k_ref[...]
    v_now = v_ref[...]
    row = lax.broadcasted_iota(jnp.int32, (WINDOW, 2 * WINDOW), 0)
    col = lax.broadcasted_iota(jnp.int32, (WINDOW, 2 * WINDOW), 1)
    distance = row + WINDOW - col
    first_col = jnp.where(head_block & (info_ref[0] == 0), WINDOW, 0)
    allowed = (distance >= 0) & (distance < WINDOW) & (col >= first_col)
    queries = q_ref[...]
    pieces = []
    for kv in range(kv_local):
        part = slice(kv * HEAD, (kv + 1) * HEAD)
        keys = jnp.concatenate([k_prev[:, part], k_now[:, part]], axis=0)
        values = jnp.concatenate([v_prev[:, part], v_now[:, part]], axis=0)
        for g in range(group_size):
            head = kv * group_size + g
            scores = lax.dot_general(
                queries[:, head * HEAD : (head + 1) * HEAD],
                keys,
                (((1,), (1,)), ((), ())),
                preferred_element_type=F32,
            ) * HEAD ** (-0.5)
            logits = jnp.where(allowed, scores, -jnp.inf)
            sink = sink_ref[head]
            top = jnp.maximum(jnp.max(logits, axis=-1, keepdims=True), sink)
            raised = jnp.exp(logits - top)
            total = jnp.sum(raised, axis=-1, keepdims=True) + jnp.exp(sink - top)
            probs = (raised * (1.0 / total)).astype(BF16)
            pieces.append(jnp.dot(probs, values, preferred_element_type=F32).astype(BF16))
    out_ref[...] = jnp.concatenate(pieces, axis=-1).reshape(out_ref.shape)


def attend(query_heads, key_heads, value_heads, sink_logit, tail, tok_rows):
    span, q_cols = query_heads.shape
    kv_cols = key_heads.shape[1]
    kv_local = kv_cols // HEAD
    group_size = q_cols // kv_cols
    blocks = span // WINDOW
    smem = pl.BlockSpec(memory_space=pltpu.SMEM)
    info = lax.axis_index("sp").astype(jnp.int32).reshape(1)
    return pl.pallas_call(
        functools.partial(attention_kernel, kv_local=kv_local, group_size=group_size),
        grid=(blocks,),
        in_specs=[
            smem,
            smem,
            pl.BlockSpec((WINDOW, q_cols), lambda n: (n, 0)),
            pl.BlockSpec((WINDOW, kv_cols), lambda n: (n, 0)),
            pl.BlockSpec((WINDOW, kv_cols), lambda n: (jnp.maximum(n - 1, 0), 0)),
            pl.BlockSpec((WINDOW, kv_cols), lambda n: (n, 0)),
            pl.BlockSpec((WINDOW, kv_cols), lambda n: (jnp.maximum(n - 1, 0), 0)),
            pl.BlockSpec((WINDOW, 2 * kv_cols), lambda n: (0, 0)),
        ],
        out_specs=pl.BlockSpec((WINDOW // tok_rows, tok_rows, q_cols), lambda n: (n, 0, 0)),
        out_shape=jax.ShapeDtypeStruct((span // tok_rows, tok_rows, q_cols), BF16),
        name="attend",
    )(info, sink_logit, query_heads, key_heads, key_heads, value_heads, value_heads, tail)


def pack(meta, normed, send_refs, index, expert_count, slots):
    for distance, send_ref in enumerate(send_refs):
        hot, _ = placement(meta, index ^ distance, expert_count)
        send_ref[...] = lax.dot_general(
            hot[:, :slots], normed, (((0,), (0,)), ((), ())), preferred_element_type=F32
        ).astype(BF16)


def project_kernel(
    info_ref, att_ref, w_ref, res_ref, gain_ref, meta_ref, stream_ref, ext_ref, *refs, expert_count, slots, tile
):
    send_refs, acc_ref = refs[:-1], refs[-1]
    sources, _, cols = att_ref.shape
    width = stream_ref.shape[1]
    for n in range(width // tile):
        part = slice(n * tile, (n + 1) * tile)
        total = None
        for k in range(sources):
            piece = jnp.dot(
                att_ref[k], w_ref[k * cols : (k + 1) * cols, part], preferred_element_type=F32
            )
            total = piece if total is None else total + piece
        acc_ref[:, part] = total
    stream = (res_ref[...].astype(F32) + acc_ref[...]).astype(BF16)
    stream_ref[...] = stream
    wide = stream.astype(F32)
    scale = lax.rsqrt(jnp.mean(wide * wide, axis=-1, keepdims=True) + eps)
    normed = (wide * scale * gain_ref[...]).astype(BF16)
    ext_ref[:, :width] = normed
    ext_ref[:, width:] = meta_ref[...]
    pack(meta_ref[...], normed, send_refs, info_ref[0], expert_count, slots)


def project(index, gathered, out_weight, residual, norm_gain, meta, expert_count, slots):
    _, rows, _ = gathered.shape
    width = out_weight.shape[1]
    whole = pl.BlockSpec(memory_space=pltpu.VMEM)
    send = jax.ShapeDtypeStruct((slots, width), BF16)
    outs = pl.pallas_call(
        functools.partial(
            project_kernel, expert_count=expert_count, slots=slots, tile=min(512, width)
        ),
        in_specs=[pl.BlockSpec(memory_space=pltpu.SMEM)] + [whole] * 5,
        out_specs=[whole] * (2 + expert_count),
        out_shape=[
            jax.ShapeDtypeStruct((rows, width), BF16),
            jax.ShapeDtypeStruct((rows, width + LANES), BF16),
        ]
        + [send] * expert_count,
        scratch_shapes=[pltpu.VMEM((rows, width), F32)],
        name="project",
    )(index, gathered, out_weight, residual, norm_gain.reshape(1, width), meta)
    return outs[0], outs[1], outs[2:]


def pack_kernel(info_ref, ext_ref, *send_refs, expert_count, slots):
    width = ext_ref.shape[1] - LANES
    pack(ext_ref[:, width:], ext_ref[:, :width], send_refs, info_ref[0], expert_count, slots)


def pack_far(index, ext, expert_count, slots):
    whole = pl.BlockSpec(memory_space=pltpu.VMEM)
    send = jax.ShapeDtypeStruct((slots, ext.shape[1] - LANES), BF16)
    return pl.pallas_call(
        functools.partial(pack_kernel, expert_count=expert_count, slots=slots),
        in_specs=[pl.BlockSpec(memory_space=pltpu.SMEM), whole],
        out_specs=[whole] * expert_count,
        out_shape=[send] * expert_count,
        name="pack_far",
    )(index, ext)


def token_meta(own_routes, route_weight, expert_count):
    chosen = own_routes[:, :, None] == jnp.arange(expert_count, dtype=jnp.int32)
    weight = jnp.sum(jnp.where(chosen, route_weight[:, :, None], 0.0), axis=1)
    terms = [jnp.any(chosen, axis=1).astype(F32)]
    for _ in range(3):
        term = lax.reduce_precision(weight, 8, 7)
        terms.append(term)
        weight = weight - term
    packed = jnp.concatenate(terms, axis=1)
    return jnp.pad(packed, ((0, 0), (0, LANES - packed.shape[1]))).astype(BF16)


def placement(meta, expert, expert_count):
    rows = meta.shape[0]
    lane = lax.broadcasted_iota(jnp.int32, meta.shape, 1)
    wide = meta.astype(F32)
    chosen = jnp.sum(jnp.where(lane == expert, wide, 0.0), axis=1, keepdims=True)
    of_weight = (lane > expert_count - 1) & (lane < 4 * expert_count)
    of_weight &= lax.rem(lane, expert_count) == expert
    weight = jnp.sum(jnp.where(of_weight, wide, 0.0), axis=1, keepdims=True)
    earlier = lax.broadcasted_iota(jnp.int32, (rows, rows), 1) < lax.broadcasted_iota(
        jnp.int32, (rows, rows), 0
    )
    before = jnp.dot(
        earlier.astype(F32).astype(BF16),
        jnp.broadcast_to(chosen, (rows, LANES)).astype(BF16),
        preferred_element_type=F32,
    )
    slot = lax.broadcasted_iota(jnp.int32, (rows, LANES), 1)
    hot = (before.astype(jnp.int32) == slot) & (chosen > 0.5)
    return hot.astype(F32).astype(BF16), weight


def gate_up_kernel(*refs, groups, slots, pieces, hid):
    row_refs, refs = refs[:groups], refs[groups:]
    gates, tops, ends = refs[:pieces], refs[pieces : 2 * pieces], refs[2 * pieces : 3 * pieces]
    hidden_ref, picked_ref, weight_ref, sems = refs[3 * pieces :]
    cut = tops[0].shape[0]
    copies = []
    for p in range(pieces):
        targets = (
            weight_ref.at[p, 0],
            weight_ref.at[p, 1, pl.ds(0, cut)],
            weight_ref.at[p, 1, pl.ds(cut, ends[p].shape[0])],
        )
        copies.append(
            [
                pltpu.make_async_copy(source, target, sems.at[p, j])
                for j, (source, target) in enumerate(zip((gates[p], tops[p], ends[p]), targets))
            ]
        )
    for group in copies:
        for copy in group:
            copy.start()
    for b in range(groups):
        picked_ref[b * slots : (b + 1) * slots, :] = row_refs[b][...]
    picked = picked_ref[...]
    for p in range(pieces):
        for copy in copies[p]:
            copy.wait()
        gate_pre = jnp.dot(picked, weight_ref[p, 0], preferred_element_type=F32)
        upward = jnp.dot(picked, weight_ref[p, 1], preferred_element_type=F32)
        capped = jnp.minimum(gate_pre, clamp_limit)
        linear = jnp.clip(upward, -clamp_limit, clamp_limit)
        hidden = capped * jax.nn.sigmoid(sigmoid_alpha * capped) * (linear + 1.0)
        hidden_ref[:, p * hid : (p + 1) * hid] = hidden.astype(BF16)


def gate_up(rows, gates, tops, ends):
    groups, pieces = len(rows), len(gates)
    slots, width = rows[0].shape
    hid = gates[0].shape[1]
    whole = pl.BlockSpec(memory_space=pltpu.VMEM)
    anywhere = pl.BlockSpec(memory_space=pl.ANY)
    return pl.pallas_call(
        functools.partial(gate_up_kernel, groups=groups, slots=slots, pieces=pieces, hid=hid),
        in_specs=[whole] * groups + [anywhere] * (3 * pieces),
        out_specs=whole,
        out_shape=jax.ShapeDtypeStruct((groups * slots, pieces * hid), BF16),
        scratch_shapes=[
            pltpu.VMEM((groups * slots, width), BF16),
            pltpu.VMEM((pieces, 2, width, hid), BF16),
            pltpu.SemaphoreType.DMA((pieces, 3)),
        ],
    )(*rows, *gates, *tops, *ends)


def down_kernel(hidden_ref, *refs, groups, slots, pieces, hid, tile):
    downs = refs[:pieces]
    out_refs = refs[pieces:]
    width = out_refs[0].shape[1]
    for n in range(width // tile):
        cols = slice(n * tile, (n + 1) * tile)
        total = None
        for p in range(pieces):
            part = jnp.dot(
                hidden_ref[:, p * hid : (p + 1) * hid],
                downs[p][:, cols],
                preferred_element_type=F32,
            )
            total = part if total is None else total + part
        expert_out = total.astype(BF16)
        for b in range(groups):
            out_refs[b][:, cols] = expert_out[b * slots : (b + 1) * slots, :]


def down(hidden, downs, groups):
    hid, width = downs[0].shape
    pieces = len(downs)
    slots = hidden.shape[0] // groups
    whole = pl.BlockSpec(memory_space=pltpu.VMEM)
    body = functools.partial(
        down_kernel, groups=groups, slots=slots, pieces=pieces, hid=hid, tile=min(512, width)
    )
    return pl.pallas_call(
        body,
        in_specs=[whole] * (1 + pieces),
        out_specs=[whole] * groups,
        out_shape=[jax.ShapeDtypeStruct((slots, width), BF16)] * groups,
    )(hidden, *downs)


def unpack(meta, back_refs, index, expert_count, slots):
    total = None
    for distance, back_ref in enumerate(back_refs):
        hot, weight = placement(meta, index ^ distance, expert_count)
        spread = jnp.dot(hot[:, :slots], back_ref[...], preferred_element_type=F32) * weight
        total = spread if total is None else total + spread
    return total


def combine_far_kernel(info_ref, meta_ref, *refs, expert_count, slots):
    refs[-1][...] = unpack(meta_ref[...], refs[:-1], info_ref[0], expert_count, slots).astype(BF16)


def combine_own_kernel(info_ref, meta_ref, stream_ref, far_ref, *refs, expert_count, slots):
    total = unpack(meta_ref[...], refs[:-1], info_ref[0], expert_count, slots)
    total += stream_ref[...].astype(F32) + far_ref[...].astype(F32)
    refs[-1][...] = total.astype(BF16)


def combine(kernel, index, ext, extra, backs):
    slots, width = backs[0].shape
    rows = ext.shape[0]
    meta_at = width // LANES
    whole = pl.BlockSpec(memory_space=pltpu.VMEM)
    return pl.pallas_call(
        functools.partial(kernel, expert_count=len(backs), slots=slots),
        grid=(1,),
        in_specs=[
            pl.BlockSpec(memory_space=pltpu.SMEM),
            pl.BlockSpec((rows, LANES), lambda i: (0, meta_at)),
        ]
        + [whole] * (len(extra) + len(backs)),
        out_specs=whole,
        out_shape=jax.ShapeDtypeStruct((rows, width), BF16),
    )(index, ext, *extra, *backs)


def layer(
    query_heads,
    key_heads,
    value_heads,
    sink_logit,
    residual,
    out_weight,
    norm_gain,
    routes,
    route_weight,
    gate_weight,
    up_weight,
    down_weight,
):
    expert_count = lax.axis_size("sp")
    half = lax.axis_size("tp") // 2
    tok_rows = residual.shape[0]
    choose_count = routes.shape[1]
    tp_index = lax.axis_index("tp")
    index = lax.axis_index("sp").astype(jnp.int32).reshape(1)

    def across(block):
        return exchange(block, "tp", lambda i: (i + half) % (2 * half))

    def to_experts(blocks):
        return [blocks[0]] + [exchange(blocks[d], "sp", lambda i, d=d: i ^ d) for d in range(1, expert_count)]

    tail = jnp.concatenate([key_heads[-WINDOW:], value_heads[-WINDOW:]], axis=1)
    tail = from_behind(tail, "sp")
    gates, downs = [gate_weight[0]], [down_weight[0]]
    tops, ends = jnp.split(up_weight[0], 2, axis=0)
    tops, ends = [tops], [ends]
    for distance in range(1, half):
        if distance % 2:
            step, source = 1, distance - 1
        else:
            step, source = distance, 0
        for held in (gates, tops, ends, downs):
            held.append(exchange(held[source], "tp", lambda i, s=step: i ^ s))

    attended = attend(query_heads, key_heads, value_heads, sink_logit, tail, tok_rows)
    gathered = lax.all_to_all(attended, "tp", split_axis=0, concat_axis=0, tiled=True)
    own_routes = lax.dynamic_slice_in_dim(routes, tp_index * tok_rows, tok_rows, 0)
    meta = token_meta(own_routes, route_weight, expert_count)

    capacity = max(2, 5 * tok_rows * choose_count // (4 * expert_count))
    slots = -(-capacity // SLOT_TILE) * SLOT_TILE
    stream, ext, send_own = project(index, gathered, out_weight, residual, norm_gain, meta, expert_count, slots)
    ext_far = across(ext)
    rows_own = to_experts(send_own)
    hidden_own = gate_up(rows_own, gates, tops, ends)
    rows_far = to_experts(pack_far(index, ext_far, expert_count, slots))
    hidden_far = gate_up(rows_far, gates, tops, ends)
    backs_far = to_experts(down(hidden_far, downs, expert_count))
    backs_own = to_experts(down(hidden_own, downs, expert_count))
    part_far = across(combine(combine_far_kernel, index, ext_far, (), backs_far))
    return combine(combine_own_kernel, index, ext, (stream, part_far), backs_own)


def solution(mesh):
    placed = (
        P("sp", "tp"),
        P("sp", "tp"),
        P("sp", "tp"),
        P("tp"),
        P(("sp", "tp"), None),
        P(),
        P(),
        P("sp", None),
        P(("sp", "tp"), None),
        P("sp", None, "tp"),
        P("sp", None, "tp"),
        P("sp", "tp", None),
    )
    return jax.shard_map(layer, mesh=mesh, in_specs=placed, out_specs=P(("sp", "tp"), None), check_vma=False)
```

```python
import functools

import jax
import jax.numpy as jnp
from jax import lax
from jax.experimental import pallas as pl
from jax.experimental.pallas import tpu as pltpu
from jax.sharding import PartitionSpec as P


HEAD = 64
WINDOW = 128
LANES = 128
SLOT_TILE = 16


eps = 1e-06
clamp_limit = 7.0
sigmoid_alpha = 1.702

F32 = jnp.float32
BF16 = jnp.bfloat16


def grant(mebibytes):
    return pltpu.CompilerParams(vmem_limit_bytes=mebibytes * 2**20)


def exchange(block, axis, partner):
    devices = range(lax.axis_size(axis))
    return lax.ppermute(block, axis, [(i, partner(i)) for i in devices])


def from_behind(block, axis):
    devices = range(lax.axis_size(axis))
    return lax.ppermute(block, axis, [(i - 1, i) for i in devices if i > 0])


def first_kernel(k_ref, v_ref, gate_ref, tail_ref, top_ref, sem):
    top = pltpu.make_async_copy(gate_ref.at[pl.ds(0, top_ref.shape[0])], top_ref, sem)
    top.start()
    kv_cols = k_ref.shape[1]
    tail_ref[:, :kv_cols] = k_ref[...]
    tail_ref[:, kv_cols:] = v_ref[...]
    top.wait()


def first_moves(key_heads, value_heads, gate):
    span, kv_cols = key_heads.shape
    last = pl.BlockSpec((WINDOW, kv_cols), lambda i: (span // WINDOW - 1, 0))
    stored = pl.BlockSpec(memory_space=pltpu.HBM)
    return pl.pallas_call(
        first_kernel,
        grid=(1,),
        in_specs=[last, last, stored],
        out_specs=[pl.BlockSpec(memory_space=pltpu.VMEM)] * 2,
        out_shape=[
            jax.ShapeDtypeStruct((WINDOW, 2 * kv_cols), BF16),
            jax.ShapeDtypeStruct((gate.shape[0] // 2, gate.shape[1]), BF16),
        ],
        scratch_shapes=[pltpu.SemaphoreType.DMA],
        name="first_moves",
    )(key_heads, value_heads, gate)


def cut_kernel(gate_ref, down_ref, end_ref, left_ref, right_ref, sems):
    rows, cols = end_ref.shape[0], left_ref.shape[1]
    copies = [
        pltpu.make_async_copy(gate_ref.at[pl.ds(rows, rows)], end_ref, sems.at[0]),
        pltpu.make_async_copy(down_ref.at[:, pl.ds(0, cols)], left_ref, sems.at[1]),
        pltpu.make_async_copy(down_ref.at[:, pl.ds(cols, cols)], right_ref, sems.at[2]),
    ]
    for copy in copies:
        copy.start()
    for copy in copies:
        copy.wait()


def cut_weights(gate, down):
    stored = pl.BlockSpec(memory_space=pltpu.HBM)
    half_down = jax.ShapeDtypeStruct((down.shape[0], down.shape[1] // 2), BF16)
    return pl.pallas_call(
        cut_kernel,
        in_specs=[stored] * 2,
        out_specs=[pl.BlockSpec(memory_space=pltpu.VMEM)] * 3,
        out_shape=[
            jax.ShapeDtypeStruct((gate.shape[0] // 2, gate.shape[1]), BF16),
            half_down,
            half_down,
        ],
        scratch_shapes=[pltpu.SemaphoreType.DMA((3,))],
        name="cut_weights",
    )(gate, down)


def attention_kernel(
    info_ref, sink_ref, q_hbm, k_hbm, v_hbm, tail_ref, out_ref, q_ref, k_ref, v_ref, kk_ref, vt_ref,
    logit_ref, spread_ref, rest_ref, sems, *, blocks, kv_local, group_size,
):
    kv_cols = kv_local * HEAD
    copies = [
        pltpu.make_async_copy(source, target, sems.at[j])
        for j, (source, target) in enumerate(((k_hbm, k_ref), (v_hbm, v_ref), (q_hbm, q_ref)))
    ]
    for copy in copies:
        copy.start()
    row = lax.broadcasted_iota(jnp.int32, (WINDOW, 2 * WINDOW), 0)
    col = lax.broadcasted_iota(jnp.int32, (WINDOW, 2 * WINDOW), 1)
    first_head = lax.broadcasted_iota(jnp.int32, (1, 2 * WINDOW), 1) < WINDOW
    before = row > lax.rem(col, WINDOW)
    low = lax.broadcasted_iota(jnp.int32, (WINDOW, 2 * HEAD), 1) < HEAD
    penalty = jnp.where(info_ref[0] == 0, -jnp.inf, 0.0)
    zeros = jnp.zeros((WINDOW, 2 * WINDOW), BF16)
    ones_rows = vt_ref.shape[1] - HEAD
    copies[0].wait()
    copies[1].wait()
    for block in range(blocks + 1):
        to = slice(block * WINDOW, (block + 1) * WINDOW)
        if block == 0:
            keys, values = tail_ref[:, :kv_cols], tail_ref[:, kv_cols:]
        else:
            at = slice((block - 1) * WINDOW, block * WINDOW)
            keys, values = k_ref[at, :], v_ref[at, :]
        turned = values.astype(F32).T.astype(BF16)
        for kv in range(kv_local):
            part = slice(kv * HEAD, (kv + 1) * HEAD)
            kk_ref[kv, to, :] = jnp.concatenate([keys[:, part], keys[:, part]], axis=1)
            vt_ref[kv, :HEAD, to] = turned[part, :]
            vt_ref[kv, HEAD:, to] = jnp.ones((ones_rows, WINDOW), BF16)
    copies[2].wait()
    per_block = out_ref.shape[0] // blocks
    pairs = kv_local * group_size // 2
    work = [(block, pair) for block in range(blocks) for pair in range(pairs)]
    for block, pair in work:
        band = slice(block * WINDOW, (block + 2) * WINDOW)
        queries = q_ref[
            block * WINDOW : (block + 1) * WINDOW, pair * 2 * HEAD : (pair + 1) * 2 * HEAD
        ] * jnp.asarray(HEAD ** (-0.5), BF16)
        blank = jnp.zeros_like(queries)
        stacked = jnp.concatenate(
            [jnp.where(low, queries, blank), jnp.where(low, blank, queries)], axis=0
        )
        scores = lax.dot_general(
            kk_ref[2 * pair // group_size, band, :],
            stacked,
            (((1,), (1,)), ((), ())),
            preferred_element_type=F32,
        )
        earlier = scores[:WINDOW, :]
        if block == 0:
            earlier = earlier + penalty
        logit_ref[block * pairs + pair] = jnp.where(before, earlier, scores[WINDOW:, :])
    for block, pair in work:
        item = block * pairs + pair
        logits = logit_ref[item]
        sink = jnp.where(first_head, sink_ref[2 * pair], sink_ref[2 * pair + 1])
        top = jnp.maximum(jnp.max(logits, axis=0, keepdims=True), sink)
        raised = jnp.exp(logits - top).astype(BF16)
        spread_ref[item, :WINDOW, :] = jnp.where(before, raised, zeros)
        spread_ref[item, WINDOW:, :] = jnp.where(before, zeros, raised)
        rest_ref[item] = jnp.broadcast_to(jnp.exp(sink - top), rest_ref.shape[1:])
    for block, pair in work:
        item = block * pairs + pair
        band = slice(block * WINDOW, (block + 2) * WINDOW)
        summed = jnp.dot(
            vt_ref[2 * pair // group_size, :, band], spread_ref[item], preferred_element_type=F32
        )
        total = summed[HEAD : HEAD + 1, :] + rest_ref[item][:1, :]
        scaled = summed[:HEAD, :] * (1.0 / total)
        turned = jnp.concatenate([scaled[:, :WINDOW], scaled[:, WINDOW:]], axis=0).T
        out_ref[
            block * per_block : (block + 1) * per_block, :, pair * 2 * HEAD : (pair + 1) * 2 * HEAD
        ] = turned.astype(BF16).reshape((per_block, out_ref.shape[1], 2 * HEAD))


def attend(query_heads, key_heads, value_heads, sink_logit, tail, tok_rows):
    span, q_cols = query_heads.shape
    kv_cols = key_heads.shape[1]
    kv_local = kv_cols // HEAD
    smem = pl.BlockSpec(memory_space=pltpu.SMEM)
    whole = pl.BlockSpec(memory_space=pltpu.VMEM)
    stored = pl.BlockSpec(memory_space=pltpu.HBM)
    items = span // WINDOW * q_cols // (2 * HEAD)
    info = lax.axis_index("sp").astype(jnp.int32).reshape(1)
    return pl.pallas_call(
        functools.partial(
            attention_kernel,
            blocks=span // WINDOW,
            kv_local=kv_local,
            group_size=q_cols // kv_cols,
        ),
        in_specs=[smem, smem] + [stored] * 3 + [whole],
        out_specs=whole,
        out_shape=jax.ShapeDtypeStruct((span // tok_rows, tok_rows, q_cols), BF16),
        scratch_shapes=[
            pltpu.VMEM((span, q_cols), BF16),
            pltpu.VMEM((span, kv_cols), BF16),
            pltpu.VMEM((span, kv_cols), BF16),
            pltpu.VMEM((kv_local, span + WINDOW, 2 * HEAD), BF16),
            pltpu.VMEM((kv_local, HEAD + SLOT_TILE, span + WINDOW), BF16),
            pltpu.VMEM((items, WINDOW, 2 * WINDOW), F32),
            pltpu.VMEM((items, 2 * WINDOW, 2 * WINDOW), BF16),
            pltpu.VMEM((items, 8, 2 * WINDOW), F32),
            pltpu.SemaphoreType.DMA((3,)),
        ],
        name="attend",
    )(info, sink_logit, query_heads, key_heads, value_heads, tail)


def slots_of(ids, expert, slots):
    choices, rows = ids.shape
    chosen = jnp.zeros((8, rows), F32)
    for k in range(choices):
        match = jnp.broadcast_to(ids[k : k + 1, :], (8, rows)) == expert
        chosen += jnp.where(match, 1.0, 0.0)
    earlier = lax.broadcasted_iota(jnp.int32, (rows, rows), 0) < lax.broadcasted_iota(
        jnp.int32, (rows, rows), 1
    )
    rank = jnp.dot(
        chosen.astype(BF16), earlier.astype(F32).astype(BF16), preferred_element_type=F32
    )
    place = jnp.where(chosen > 0.5, rank, -1.0).astype(jnp.int32)
    return lax.broadcasted_iota(jnp.int32, (slots, rows), 0) == place[:1, :]


def gather_kernel(info_ref, ids_ref, gather_ref, *, expert_count, slots):
    for block in range(ids_ref.shape[0]):
        for distance in range(expert_count):
            hot = slots_of(ids_ref[block], info_ref[0] ^ distance, slots)
            gather_ref[block, distance] = hot.astype(F32).astype(BF16)


def spread_kernel(info_ref, ids_ref, *refs, expert_count, slots):
    weight_refs, spread_ref = refs[:-1], refs[-1]
    blocks, choices, rows = ids_ref.shape
    for block in range(blocks):
        ids = ids_ref[block]
        for distance in range(expert_count):
            expert = info_ref[0] ^ distance
            weight = jnp.zeros((1, rows), F32)
            for k in range(choices):
                match = ids[k : k + 1, :] == expert
                weight += jnp.where(match, weight_refs[block][k : k + 1, :], 0.0)
            weight = jnp.where(slots_of(ids, expert, LANES), weight, 0.0).T
            high = weight.astype(BF16)
            spread_ref[block, distance, 0] = high
            spread_ref[block, distance, 1] = (weight - high.astype(F32)).astype(BF16)


def table(kernel, operands, shape, expert_count, slots):
    whole = pl.BlockSpec(memory_space=pltpu.VMEM)
    return pl.pallas_call(
        functools.partial(kernel, expert_count=expert_count, slots=slots),
        in_specs=[pl.BlockSpec(memory_space=pltpu.SMEM)] + [whole] * (len(operands) - 1),
        out_specs=whole,
        out_shape=jax.ShapeDtypeStruct(shape, BF16),
        compiler_params=grant(4),
    )(*operands)


def pack(gather_ref, normed, send_refs):
    for distance, send_ref in enumerate(send_refs):
        send_ref[...] = jnp.dot(
            gather_ref[0, distance], normed, preferred_element_type=F32
        ).astype(BF16)


def project_kernel(
    att_ref, w_hbm, res_ref, gain_ref, gather_ref, stream_ref, *refs, expert_count, parts, tile
):
    part_refs, send_refs = refs[:parts], refs[parts:-3]
    acc_ref, w_ref, sems = refs[-3:]
    sources, _, cols = att_ref.shape
    width = stream_ref.shape[1]
    copies = []
    for n in range(width // tile):
        part = pl.ds(n * tile, tile)
        copies.append(pltpu.make_async_copy(w_hbm.at[:, part], w_ref.at[n], sems.at[n]))
    for copy in copies:
        copy.start()
    for n in range(width // tile):
        copies[n].wait()
        total = None
        for k in range(sources):
            piece = jnp.dot(
                att_ref[k], w_ref[n, k * cols : (k + 1) * cols, :], preferred_element_type=F32
            )
            total = piece if total is None else total + piece
        acc_ref[:, n * tile : (n + 1) * tile] = total
    stream = (res_ref[...].astype(F32) + acc_ref[...]).astype(BF16)
    stream_ref[...] = stream
    wide = stream.astype(F32)
    scale = lax.rsqrt(jnp.mean(wide * wide, axis=-1, keepdims=True) + eps)
    normed = (wide * scale * gain_ref[...]).astype(BF16)
    step = width // parts
    for h in range(parts):
        part_refs[h][...] = normed[:, h * step : (h + 1) * step]
    pack(gather_ref, normed, send_refs)


def block_of(array, block):
    zeros = (0,) * (array.ndim - 1)
    return pl.BlockSpec((1,) + array.shape[1:], lambda i: (block,) + zeros)


def project(gathered, out_weight, residual, norm_gain, gather, parts):
    _, rows, _ = gathered.shape
    width = out_weight.shape[1]
    _, expert_count, slots, _ = gather.shape
    tile = min(512, width)
    whole = pl.BlockSpec(memory_space=pltpu.VMEM)
    outs = pl.pallas_call(
        functools.partial(
            project_kernel, expert_count=expert_count, parts=parts, tile=tile
        ),
        grid=(1,),
        in_specs=[whole, pl.BlockSpec(memory_space=pltpu.HBM), whole, whole, block_of(gather, 0)],
        out_specs=[whole] * (1 + parts + expert_count),
        out_shape=[jax.ShapeDtypeStruct((rows, width), BF16)]
        + [jax.ShapeDtypeStruct((rows, width // parts), BF16)] * parts
        + [jax.ShapeDtypeStruct((slots, width), BF16)] * expert_count,
        scratch_shapes=[
            pltpu.VMEM((rows, width), F32),
            pltpu.VMEM((width // tile, out_weight.shape[0], tile), BF16),
            pltpu.SemaphoreType.DMA((width // tile,)),
        ],
        name="project",
    )(gathered, out_weight, residual, norm_gain, gather)
    return outs[0], outs[1 : 1 + parts], outs[1 + parts :]


def pack_kernel(gather_ref, far_ref, *send_refs):
    pack(gather_ref, far_ref[...], send_refs)


def pack_far(gather, far):
    _, expert_count, slots, _ = gather.shape
    whole = pl.BlockSpec(memory_space=pltpu.VMEM)
    return pl.pallas_call(
        pack_kernel,
        grid=(1,),
        in_specs=[block_of(gather, 1), whole],
        out_specs=[whole] * expert_count,
        out_shape=[jax.ShapeDtypeStruct((slots, far.shape[1]), BF16)] * expert_count,
        compiler_params=grant(4),
        name="pack_far",
    )(gather, far)


def gate_up_kernel(*refs, groups, parts, slots, pieces, hid, chunks):
    row_refs, refs = refs[: groups * parts], refs[groups * parts :]
    count = sum(chunks)
    gate_refs, ups = refs[:count], refs[count : count + pieces]
    hidden_ref, picked_ref, weight_ref, sems = refs[count + pieces :]
    copies, at = [], 0
    for p in range(pieces):
        group, row = [], 0
        for chunk in gate_refs[at : at + chunks[p]]:
            target = weight_ref.at[p, 0, pl.ds(row, chunk.shape[0])]
            group.append(pltpu.make_async_copy(chunk, target, sems.at[p, len(group)]))
            row += chunk.shape[0]
        at += chunks[p]
        group.append(pltpu.make_async_copy(ups[p], weight_ref.at[p, 1], sems.at[p, len(group)]))
        copies.append(group)
    for group in copies:
        for copy in group:
            copy.start()
    step = picked_ref.shape[1] // parts
    for b in range(groups):
        for h in range(parts):
            rows = row_refs[h * groups + b][...]
            picked_ref[b * slots : (b + 1) * slots, h * step : (h + 1) * step] = rows
    picked = picked_ref[...]
    for p in range(pieces):
        for copy in copies[p]:
            copy.wait()
        gate_pre = jnp.dot(picked, weight_ref[p, 0], preferred_element_type=F32)
        upward = jnp.dot(picked, weight_ref[p, 1], preferred_element_type=F32)
        capped = jnp.minimum(gate_pre, clamp_limit)
        linear = jnp.clip(upward, -clamp_limit, clamp_limit)
        hidden = capped * jax.nn.sigmoid(sigmoid_alpha * capped) * (linear + 1.0)
        hidden_ref[:, p * hid : (p + 1) * hid] = hidden.astype(BF16)


def gate_up(rows, parts, gates, ups):
    groups, pieces = len(rows) // parts, len(gates)
    slots = rows[0].shape[0]
    width, hid = ups[0].shape
    chunks = tuple(len(piece) for piece in gates)
    flat = [chunk for piece in gates for chunk in piece]
    whole = pl.BlockSpec(memory_space=pltpu.VMEM)
    stored = pl.BlockSpec(memory_space=pltpu.HBM)
    return pl.pallas_call(
        functools.partial(
            gate_up_kernel,
            groups=groups,
            parts=parts,
            slots=slots,
            pieces=pieces,
            hid=hid,
            chunks=chunks,
        ),
        in_specs=[whole] * len(rows) + [stored] * (len(flat) + pieces),
        out_specs=whole,
        out_shape=jax.ShapeDtypeStruct((groups * slots, pieces * hid), BF16),
        scratch_shapes=[
            pltpu.VMEM((groups * slots, width), BF16),
            pltpu.VMEM((pieces, 2, width, hid), BF16),
            pltpu.SemaphoreType.DMA((pieces, max(chunks) + 1)),
        ],
        compiler_params=grant(20),
    )(*rows, *flat, *ups)


def down_kernel(hidden_ref, *refs, groups, slots, hid, chunks, tile):
    out_refs = refs[sum(chunks) :]
    width = out_refs[0].shape[1]
    for n in range(width // tile):
        total, at = None, 0
        for p, count in enumerate(chunks):
            ref = refs[at + n * tile * count // width]
            start = n * tile % (width // count)
            at += count
            part = jnp.dot(
                hidden_ref[:, p * hid : (p + 1) * hid],
                ref[:, start : start + tile],
                preferred_element_type=F32,
            )
            total = part if total is None else total + part
        expert_out = total.astype(BF16)
        for b in range(groups):
            out_refs[b][:, n * tile : (n + 1) * tile] = expert_out[b * slots : (b + 1) * slots, :]


def down(hidden, downs, groups, part, parts):
    hid = downs[0][0].shape[0]
    full = sum(chunk.shape[1] for chunk in downs[0])
    width = full // parts
    slots = hidden.shape[0] // groups
    whole = pl.BlockSpec(memory_space=pltpu.VMEM)
    operands, specs, chunks = [], [], []
    for piece in downs:
        if len(piece) == 1:
            operands.append(piece[0])
            specs.append(pl.BlockSpec((hid, width), lambda i: (0, part)))
            chunks.append(1)
        else:
            used = piece[part * len(piece) // parts : (part + 1) * len(piece) // parts]
            operands += used
            specs += [whole] * len(used)
            chunks.append(len(used))
    body = functools.partial(
        down_kernel,
        groups=groups,
        slots=slots,
        hid=hid,
        chunks=tuple(chunks),
        tile=min(512, width),
    )
    return pl.pallas_call(
        body,
        grid=(1,),
        in_specs=[whole] + specs,
        out_specs=[whole] * groups,
        out_shape=[jax.ShapeDtypeStruct((slots, width), BF16)] * groups,
        compiler_params=grant(12),
    )(hidden, *operands)


def unpack(spread_ref, back_refs):
    slots = back_refs[0].shape[0]
    total = None
    for term in (1, 0):
        for distance, back_ref in enumerate(back_refs):
            part = jnp.dot(
                spread_ref[0, distance, term][:, :slots], back_ref[...], preferred_element_type=F32
            )
            total = part if total is None else total + part
    return total


def combine_far_kernel(spread_ref, *refs):
    refs[-1][...] = unpack(spread_ref, refs[:-1]).astype(BF16)


def combine_own_kernel(spread_ref, stream_ref, *refs, parts):
    far_refs, back_refs, out_ref = refs[:parts], refs[parts:-1], refs[-1]
    total = unpack(spread_ref, back_refs) + stream_ref[...].astype(F32)
    step = total.shape[1] // parts
    for h in range(parts):
        cols = slice(h * step, (h + 1) * step)
        out_ref[:, cols] = (total[:, cols] + far_refs[h][...].astype(F32)).astype(BF16)


def combine(kernel, spread, block, extra, backs):
    rows = spread.shape[3]
    whole = pl.BlockSpec(memory_space=pltpu.VMEM)
    return pl.pallas_call(
        kernel,
        grid=(1,),
        in_specs=[block_of(spread, block)] + [whole] * (len(extra) + len(backs)),
        out_specs=whole,
        out_shape=jax.ShapeDtypeStruct((rows, backs[0].shape[1]), BF16),
        compiler_params=grant(10),
    )(spread, *extra, *backs)


def layer(
    query_heads,
    key_heads,
    value_heads,
    sink_logit,
    residual,
    out_weight,
    norm_gain,
    routes,
    route_weight,
    gate_weight,
    up_weight,
    down_weight,
):
    expert_count = lax.axis_size("sp")
    half = lax.axis_size("tp") // 2
    tok_rows = residual.shape[0]
    choose_count = routes.shape[1]
    parts = parts_of(expert_count)
    tp_index = lax.axis_index("tp")
    index = lax.axis_index("sp").astype(jnp.int32).reshape(1)

    def across(block):
        return exchange(block, "tp", lambda i: (i + half) % (2 * half))

    def to_experts(blocks):
        return [blocks[0]] + [
            exchange(blocks[d], "sp", lambda i, d=d: i ^ d)
            for d in range(1, expert_count)
        ]

    own_gate, own_up, own_down = gate_weight[0], up_weight[0], down_weight[0]
    tail, top = first_moves(key_heads, value_heads, own_gate)
    tail = from_behind(tail, "sp")
    end, left, right = cut_weights(own_gate, own_down)
    gates, ups, downs = [[own_gate]], [[own_up]], [[own_down]]
    own_chunks = {"gate": [top, end], "up": [own_up], "down": [left, right]}
    for distance in range(1, half):
        for what, held in (("gate", gates), ("up", ups), ("down", downs)):
            if distance % 2:
                step, chunks = 1, held[distance - 1]
            else:
                step, chunks = distance, own_chunks[what]
            held.append([exchange(chunk, "tp", lambda i, s=step: i ^ s) for chunk in chunks])
    ups = [piece[0] for piece in ups]

    attended = attend(query_heads, key_heads, value_heads, sink_logit, tail, tok_rows)
    gathered = lax.all_to_all(attended, "tp", split_axis=0, concat_axis=0, tiled=True)

    capacity = max(2, 5 * tok_rows * choose_count // (4 * expert_count))
    slots = -(-capacity // SLOT_TILE) * SLOT_TILE
    starts = [tp_index * tok_rows, (tp_index + half) % (2 * half) * tok_rows]
    ids = jnp.stack([lax.dynamic_slice_in_dim(routes.T, at, tok_rows, 1) for at in starts])
    weight_own = route_weight.T
    weight_far = across(weight_own)
    gather = table(
        gather_kernel, (index, ids), (2, expert_count, slots, tok_rows), expert_count, slots
    )
    spread = table(
        spread_kernel,
        (index, ids, weight_own, weight_far),
        (2, expert_count, 2, tok_rows, LANES),
        expert_count,
        slots,
    )

    stream, normed, send_own = project(
        gathered, out_weight, residual, norm_gain.reshape(1, -1), gather, parts
    )
    rows_far = []
    for h in range(parts):
        far = across(normed[h])
        rows_far += to_experts(pack_far(gather, far))
    rows_own = to_experts(send_own)
    hidden_own = gate_up(rows_own, 1, gates, ups)
    hidden_far = gate_up(rows_far, parts, gates, ups)
    part_far = []
    for h in range(parts):
        backs = down(hidden_far, downs, expert_count, h, parts)
        backs = to_experts(backs)
        mixed = combine(combine_far_kernel, spread, 1, (), backs)
        part_far.append(across(mixed))
    backs = down(hidden_own, downs, expert_count, 0, 1)
    backs = to_experts(backs)
    return combine(
        functools.partial(combine_own_kernel, parts=parts), spread, 0, (stream, *part_far), backs
    )


def parts_of(expert_count):
    return 2 if expert_count <= 4 else 1


def solution(mesh):
    placed = (
        P("sp", "tp"),
        P("sp", "tp"),
        P("sp", "tp"),
        P("tp"),
        P(("sp", "tp"), None),
        P(),
        P(),
        P("sp", None),
        P(("sp", "tp"), None),
        P("sp", None, "tp"),
        P("sp", None, "tp"),
        P("sp", "tp", None),
    )
    return jax.shard_map(
        layer, mesh=mesh, in_specs=placed, out_specs=P(("sp", "tp"), None), check_vma=False
    )
```

```python
import functools

import jax
import jax.numpy as jnp
from jax import lax
from jax.experimental import pallas as pl
from jax.experimental.pallas import tpu as pltpu
from jax.sharding import PartitionSpec as P


HEAD = 64
WINDOW = 128
LANES = 128
SLOT_TILE = 16


eps = 1e-06
clamp_limit = 7.0
sigmoid_alpha = 1.702

F32 = jnp.float32
BF16 = jnp.bfloat16


def grant(mebibytes):
    return pltpu.CompilerParams(vmem_limit_bytes=mebibytes * 2**20)


def exchange(block, axis, partner):
    devices = range(lax.axis_size(axis))
    return lax.ppermute(block, axis, [(i, partner(i)) for i in devices])


def from_behind(block, axis):
    devices = range(lax.axis_size(axis))
    return lax.ppermute(block, axis, [(i - 1, i) for i in devices if i > 0])


def first_kernel(k_ref, v_ref, tail_ref):
    kv_cols = k_ref.shape[1]
    tail_ref[:, :kv_cols] = k_ref[...]
    tail_ref[:, kv_cols:] = v_ref[...]


def first_moves(key_heads, value_heads):
    span, kv_cols = key_heads.shape
    last = pl.BlockSpec((WINDOW, kv_cols), lambda i: (span // WINDOW - 1, 0))
    return pl.pallas_call(
        first_kernel,
        grid=(1,),
        in_specs=[last, last],
        out_specs=pl.BlockSpec(memory_space=pltpu.VMEM),
        out_shape=jax.ShapeDtypeStruct((WINDOW, 2 * kv_cols), BF16),
        name="first_moves",
    )(key_heads, value_heads)


def cut_kernel(down_ref, left_ref, right_ref, sems):
    cols = left_ref.shape[1]
    copies = [
        pltpu.make_async_copy(down_ref.at[:, pl.ds(0, cols)], left_ref, sems.at[0]),
        pltpu.make_async_copy(down_ref.at[:, pl.ds(cols, cols)], right_ref, sems.at[1]),
    ]
    for copy in copies:
        copy.start()
    for copy in copies:
        copy.wait()


def cut_weight(down):
    half_down = jax.ShapeDtypeStruct((down.shape[0], down.shape[1] // 2), BF16)
    return pl.pallas_call(
        cut_kernel,
        in_specs=[pl.BlockSpec(memory_space=pltpu.HBM)],
        out_specs=[pl.BlockSpec(memory_space=pltpu.VMEM)] * 2,
        out_shape=[half_down, half_down],
        scratch_shapes=[pltpu.SemaphoreType.DMA((2,))],
        name="cut_weight",
    )(down)


def attention_kernel(
    info_ref, sink_ref, q_hbm, k_hbm, v_hbm, tail_ref, out_ref, q_ref, k_ref, v_ref, kk_ref, vt_ref,
    logit_ref, spread_ref, rest_ref, sems, *, blocks, kv_local, group_size,
):
    kv_cols = kv_local * HEAD
    copies = [
        pltpu.make_async_copy(source, target, sems.at[j])
        for j, (source, target) in enumerate(((k_hbm, k_ref), (v_hbm, v_ref), (q_hbm, q_ref)))
    ]
    for copy in copies:
        copy.start()
    row = lax.broadcasted_iota(jnp.int32, (WINDOW, 2 * WINDOW), 0)
    col = lax.broadcasted_iota(jnp.int32, (WINDOW, 2 * WINDOW), 1)
    first_head = lax.broadcasted_iota(jnp.int32, (1, 2 * WINDOW), 1) < WINDOW
    before = row > lax.rem(col, WINDOW)
    low = lax.broadcasted_iota(jnp.int32, (WINDOW, 2 * HEAD), 1) < HEAD
    penalty = jnp.where(info_ref[0] == 0, -jnp.inf, 0.0)
    zeros = jnp.zeros((WINDOW, 2 * WINDOW), BF16)
    ones_rows = vt_ref.shape[1] - HEAD
    copies[0].wait()
    copies[1].wait()
    for block in range(blocks + 1):
        to = slice(block * WINDOW, (block + 1) * WINDOW)
        if block == 0:
            keys, values = tail_ref[:, :kv_cols], tail_ref[:, kv_cols:]
        else:
            at = slice((block - 1) * WINDOW, block * WINDOW)
            keys, values = k_ref[at, :], v_ref[at, :]
        turned = values.astype(F32).T.astype(BF16)
        for kv in range(kv_local):
            part = slice(kv * HEAD, (kv + 1) * HEAD)
            kk_ref[kv, to, :] = jnp.concatenate([keys[:, part], keys[:, part]], axis=1)
            vt_ref[kv, :HEAD, to] = turned[part, :]
            vt_ref[kv, HEAD:, to] = jnp.ones((ones_rows, WINDOW), BF16)
    copies[2].wait()
    per_block = out_ref.shape[0] // blocks
    pairs = kv_local * group_size // 2
    work = [(block, pair) for block in range(blocks) for pair in range(pairs)]
    for block, pair in work:
        band = slice(block * WINDOW, (block + 2) * WINDOW)
        queries = q_ref[
            block * WINDOW : (block + 1) * WINDOW, pair * 2 * HEAD : (pair + 1) * 2 * HEAD
        ] * jnp.asarray(HEAD ** (-0.5), BF16)
        blank = jnp.zeros_like(queries)
        stacked = jnp.concatenate(
            [jnp.where(low, queries, blank), jnp.where(low, blank, queries)], axis=0
        )
        scores = lax.dot_general(
            kk_ref[2 * pair // group_size, band, :],
            stacked,
            (((1,), (1,)), ((), ())),
            preferred_element_type=F32,
        )
        earlier = scores[:WINDOW, :]
        if block == 0:
            earlier = earlier + penalty
        logit_ref[block * pairs + pair] = jnp.where(before, earlier, scores[WINDOW:, :])
    for block, pair in work:
        item = block * pairs + pair
        logits = logit_ref[item]
        sink = jnp.where(first_head, sink_ref[2 * pair], sink_ref[2 * pair + 1])
        top = jnp.maximum(jnp.max(logits, axis=0, keepdims=True), sink)
        raised = jnp.exp(logits - top).astype(BF16)
        spread_ref[item, :WINDOW, :] = jnp.where(before, raised, zeros)
        spread_ref[item, WINDOW:, :] = jnp.where(before, zeros, raised)
        rest_ref[item] = jnp.broadcast_to(jnp.exp(sink - top), rest_ref.shape[1:])
    for block, pair in work:
        item = block * pairs + pair
        band = slice(block * WINDOW, (block + 2) * WINDOW)
        summed = jnp.dot(
            vt_ref[2 * pair // group_size, :, band], spread_ref[item], preferred_element_type=F32
        )
        total = summed[HEAD : HEAD + 1, :] + rest_ref[item][:1, :]
        scaled = summed[:HEAD, :] * (1.0 / total)
        turned = jnp.concatenate([scaled[:, :WINDOW], scaled[:, WINDOW:]], axis=0).T
        out_ref[
            block * per_block : (block + 1) * per_block, :, pair * 2 * HEAD : (pair + 1) * 2 * HEAD
        ] = turned.astype(BF16).reshape((per_block, out_ref.shape[1], 2 * HEAD))


def attend(query_heads, key_heads, value_heads, sink_logit, tail, tok_rows):
    span, q_cols = query_heads.shape
    kv_cols = key_heads.shape[1]
    kv_local = kv_cols // HEAD
    smem = pl.BlockSpec(memory_space=pltpu.SMEM)
    whole = pl.BlockSpec(memory_space=pltpu.VMEM)
    stored = pl.BlockSpec(memory_space=pltpu.HBM)
    items = span // WINDOW * q_cols // (2 * HEAD)
    info = lax.axis_index("sp").astype(jnp.int32).reshape(1)
    return pl.pallas_call(
        functools.partial(
            attention_kernel,
            blocks=span // WINDOW,
            kv_local=kv_local,
            group_size=q_cols // kv_cols,
        ),
        in_specs=[smem, smem] + [stored] * 3 + [whole],
        out_specs=whole,
        out_shape=jax.ShapeDtypeStruct((span // tok_rows, tok_rows, q_cols), BF16),
        scratch_shapes=[
            pltpu.VMEM((span, q_cols), BF16),
            pltpu.VMEM((span, kv_cols), BF16),
            pltpu.VMEM((span, kv_cols), BF16),
            pltpu.VMEM((kv_local, span + WINDOW, 2 * HEAD), BF16),
            pltpu.VMEM((kv_local, HEAD + SLOT_TILE, span + WINDOW), BF16),
            pltpu.VMEM((items, WINDOW, 2 * WINDOW), F32),
            pltpu.VMEM((items, 2 * WINDOW, 2 * WINDOW), BF16),
            pltpu.VMEM((items, 8, 2 * WINDOW), F32),
            pltpu.SemaphoreType.DMA((3,)),
        ],
        name="attend",
    )(info, sink_logit, query_heads, key_heads, value_heads, tail)


def slots_of(ids, expert, slots):
    choices, rows = ids.shape
    chosen = jnp.zeros((8, rows), F32)
    for k in range(choices):
        match = jnp.broadcast_to(ids[k : k + 1, :], (8, rows)) == expert
        chosen += jnp.where(match, 1.0, 0.0)
    earlier = lax.broadcasted_iota(jnp.int32, (rows, rows), 0) < lax.broadcasted_iota(
        jnp.int32, (rows, rows), 1
    )
    rank = jnp.dot(
        chosen.astype(BF16), earlier.astype(F32).astype(BF16), preferred_element_type=F32
    )
    place = jnp.where(chosen > 0.5, rank, -1.0).astype(jnp.int32)
    return lax.broadcasted_iota(jnp.int32, (slots, rows), 0) == place[:1, :]


def gather_kernel(info_ref, ids_ref, gather_ref, *, expert_count, slots):
    for block in range(ids_ref.shape[0]):
        for distance in range(expert_count):
            hot = slots_of(ids_ref[block], info_ref[0] ^ distance, slots)
            gather_ref[block, distance] = hot.astype(F32).astype(BF16)


def spread_kernel(info_ref, ids_ref, *refs, expert_count, slots):
    weight_refs, spread_ref = refs[:-1], refs[-1]
    blocks, choices, rows = ids_ref.shape
    for block in range(blocks):
        ids = ids_ref[block]
        for distance in range(expert_count):
            expert = info_ref[0] ^ distance
            weight = jnp.zeros((1, rows), F32)
            for k in range(choices):
                match = ids[k : k + 1, :] == expert
                weight += jnp.where(match, weight_refs[block][k : k + 1, :], 0.0)
            weight = jnp.where(slots_of(ids, expert, LANES), weight, 0.0).T
            high = weight.astype(BF16)
            spread_ref[block, distance, 0] = high
            spread_ref[block, distance, 1] = (weight - high.astype(F32)).astype(BF16)


def table(kernel, operands, shape, expert_count, slots):
    whole = pl.BlockSpec(memory_space=pltpu.VMEM)
    return pl.pallas_call(
        functools.partial(kernel, expert_count=expert_count, slots=slots),
        in_specs=[pl.BlockSpec(memory_space=pltpu.SMEM)] + [whole] * (len(operands) - 1),
        out_specs=whole,
        out_shape=jax.ShapeDtypeStruct(shape, BF16),
        compiler_params=grant(4),
    )(*operands)


def pack(gather_ref, normed, send_refs):
    for distance, send_ref in enumerate(send_refs):
        send_ref[...] = jnp.dot(
            gather_ref[0, distance], normed, preferred_element_type=F32
        ).astype(BF16)


def project_kernel(
    att_ref, w_hbm, res_ref, gain_ref, gather_ref, stream_ref, *refs, expert_count, parts, tile
):
    part_refs, send_refs = refs[:parts], refs[parts:-3]
    acc_ref, w_ref, sems = refs[-3:]
    sources, _, cols = att_ref.shape
    width = stream_ref.shape[1]
    copies = []
    for n in range(width // tile):
        part = pl.ds(n * tile, tile)
        copies.append(pltpu.make_async_copy(w_hbm.at[:, part], w_ref.at[n], sems.at[n]))
    for copy in copies:
        copy.start()
    for n in range(width // tile):
        copies[n].wait()
        total = None
        for k in range(sources):
            piece = jnp.dot(
                att_ref[k], w_ref[n, k * cols : (k + 1) * cols, :], preferred_element_type=F32
            )
            total = piece if total is None else total + piece
        acc_ref[:, n * tile : (n + 1) * tile] = total
    stream = (res_ref[...].astype(F32) + acc_ref[...]).astype(BF16)
    stream_ref[...] = stream
    wide = stream.astype(F32)
    scale = lax.rsqrt(jnp.mean(wide * wide, axis=-1, keepdims=True) + eps)
    normed = (wide * scale * gain_ref[...]).astype(BF16)
    step = width // parts
    for h in range(parts):
        part_refs[h][...] = normed[:, h * step : (h + 1) * step]
    pack(gather_ref, normed, send_refs)


def block_of(array, block):
    zeros = (0,) * (array.ndim - 1)
    return pl.BlockSpec((1,) + array.shape[1:], lambda i: (block,) + zeros)


def project(gathered, out_weight, residual, norm_gain, gather, parts):
    _, rows, _ = gathered.shape
    width = out_weight.shape[1]
    _, expert_count, slots, _ = gather.shape
    tile = min(512, width)
    whole = pl.BlockSpec(memory_space=pltpu.VMEM)
    outs = pl.pallas_call(
        functools.partial(
            project_kernel, expert_count=expert_count, parts=parts, tile=tile
        ),
        grid=(1,),
        in_specs=[whole, pl.BlockSpec(memory_space=pltpu.HBM), whole, whole, block_of(gather, 0)],
        out_specs=[whole] * (1 + parts + expert_count),
        out_shape=[jax.ShapeDtypeStruct((rows, width), BF16)]
        + [jax.ShapeDtypeStruct((rows, width // parts), BF16)] * parts
        + [jax.ShapeDtypeStruct((slots, width), BF16)] * expert_count,
        scratch_shapes=[
            pltpu.VMEM((rows, width), F32),
            pltpu.VMEM((width // tile, out_weight.shape[0], tile), BF16),
            pltpu.SemaphoreType.DMA((width // tile,)),
        ],
        name="project",
    )(gathered, out_weight, residual, norm_gain, gather)
    return outs[0], outs[1 : 1 + parts], outs[1 + parts :]


def pack_kernel(gather_ref, far_ref, *send_refs):
    pack(gather_ref, far_ref[...], send_refs)


def pack_far(gather, far):
    _, expert_count, slots, _ = gather.shape
    whole = pl.BlockSpec(memory_space=pltpu.VMEM)
    return pl.pallas_call(
        pack_kernel,
        grid=(1,),
        in_specs=[block_of(gather, 1), whole],
        out_specs=[whole] * expert_count,
        out_shape=[jax.ShapeDtypeStruct((slots, far.shape[1]), BF16)] * expert_count,
        compiler_params=grant(4),
        name="pack_far",
    )(gather, far)


def gate_up_kernel(*refs, groups, parts, slots, pieces, hid, chunks):
    row_refs, refs = refs[: groups * parts], refs[groups * parts :]
    count = sum(chunks)
    gate_refs, ups = refs[:count], refs[count : count + pieces]
    hidden_ref, picked_ref, weight_ref, sems = refs[count + pieces :]
    copies, at = [], 0
    for p in range(pieces):
        group, row = [], 0
        for chunk in gate_refs[at : at + chunks[p]]:
            target = weight_ref.at[p, 0, pl.ds(row, chunk.shape[0])]
            group.append(pltpu.make_async_copy(chunk, target, sems.at[p, len(group)]))
            row += chunk.shape[0]
        at += chunks[p]
        group.append(pltpu.make_async_copy(ups[p], weight_ref.at[p, 1], sems.at[p, len(group)]))
        copies.append(group)
    for group in copies:
        for copy in group:
            copy.start()
    step = picked_ref.shape[1] // parts
    for b in range(groups):
        for h in range(parts):
            rows = row_refs[h * groups + b][...]
            picked_ref[b * slots : (b + 1) * slots, h * step : (h + 1) * step] = rows
    picked = picked_ref[...]
    for p in range(pieces):
        for copy in copies[p]:
            copy.wait()
        gate_pre = jnp.dot(picked, weight_ref[p, 0], preferred_element_type=F32)
        upward = jnp.dot(picked, weight_ref[p, 1], preferred_element_type=F32)
        capped = jnp.minimum(gate_pre, clamp_limit)
        linear = jnp.clip(upward, -clamp_limit, clamp_limit)
        hidden = capped * jax.nn.sigmoid(sigmoid_alpha * capped) * (linear + 1.0)
        hidden_ref[:, p * hid : (p + 1) * hid] = hidden.astype(BF16)


def gate_up(rows, parts, gates, ups):
    groups, pieces = len(rows) // parts, len(gates)
    slots = rows[0].shape[0]
    width, hid = ups[0].shape
    chunks = tuple(len(piece) for piece in gates)
    flat = [chunk for piece in gates for chunk in piece]
    whole = pl.BlockSpec(memory_space=pltpu.VMEM)
    stored = pl.BlockSpec(memory_space=pltpu.HBM)
    return pl.pallas_call(
        functools.partial(
            gate_up_kernel,
            groups=groups,
            parts=parts,
            slots=slots,
            pieces=pieces,
            hid=hid,
            chunks=chunks,
        ),
        in_specs=[whole] * len(rows) + [stored] * (len(flat) + pieces),
        out_specs=whole,
        out_shape=jax.ShapeDtypeStruct((groups * slots, pieces * hid), BF16),
        scratch_shapes=[
            pltpu.VMEM((groups * slots, width), BF16),
            pltpu.VMEM((pieces, 2, width, hid), BF16),
            pltpu.SemaphoreType.DMA((pieces, max(chunks) + 1)),
        ],
        compiler_params=grant(20),
    )(*rows, *flat, *ups)


def down_kernel(hidden_ref, *refs, groups, slots, hid, chunks, tile):
    out_refs = refs[sum(chunks) :]
    width = out_refs[0].shape[1]
    for n in range(width // tile):
        total, at = None, 0
        for p, count in enumerate(chunks):
            ref = refs[at + n * tile * count // width]
            start = n * tile % (width // count)
            at += count
            part = jnp.dot(
                hidden_ref[:, p * hid : (p + 1) * hid],
                ref[:, start : start + tile],
                preferred_element_type=F32,
            )
            total = part if total is None else total + part
        expert_out = total.astype(BF16)
        for b in range(groups):
            out_refs[b][:, n * tile : (n + 1) * tile] = expert_out[b * slots : (b + 1) * slots, :]


def down(hidden, downs, groups, part, parts):
    hid = downs[0][0].shape[0]
    full = sum(chunk.shape[1] for chunk in downs[0])
    width = full // parts
    slots = hidden.shape[0] // groups
    whole = pl.BlockSpec(memory_space=pltpu.VMEM)
    operands, specs, chunks = [], [], []
    for piece in downs:
        if len(piece) == 1:
            operands.append(piece[0])
            specs.append(pl.BlockSpec((hid, width), lambda i: (0, part)))
            chunks.append(1)
        else:
            used = piece[part * len(piece) // parts : (part + 1) * len(piece) // parts]
            operands += used
            specs += [whole] * len(used)
            chunks.append(len(used))
    body = functools.partial(
        down_kernel,
        groups=groups,
        slots=slots,
        hid=hid,
        chunks=tuple(chunks),
        tile=min(512, width),
    )
    return pl.pallas_call(
        body,
        grid=(1,),
        in_specs=[whole] + specs,
        out_specs=[whole] * groups,
        out_shape=[jax.ShapeDtypeStruct((slots, width), BF16)] * groups,
        compiler_params=grant(12),
    )(hidden, *operands)


def unpack(spread_ref, back_refs):
    slots = back_refs[0].shape[0]
    total = None
    for term in (1, 0):
        for distance, back_ref in enumerate(back_refs):
            part = jnp.dot(
                spread_ref[0, distance, term][:, :slots], back_ref[...], preferred_element_type=F32
            )
            total = part if total is None else total + part
    return total


def combine_far_kernel(spread_ref, *refs):
    refs[-1][...] = unpack(spread_ref, refs[:-1]).astype(BF16)


def combine_own_kernel(spread_ref, stream_ref, *refs, parts):
    far_refs, back_refs, out_ref = refs[:parts], refs[parts:-1], refs[-1]
    total = unpack(spread_ref, back_refs) + stream_ref[...].astype(F32)
    step = total.shape[1] // parts
    for h in range(parts):
        cols = slice(h * step, (h + 1) * step)
        out_ref[:, cols] = (total[:, cols] + far_refs[h][...].astype(F32)).astype(BF16)


def combine(kernel, spread, block, extra, backs):
    rows = spread.shape[3]
    whole = pl.BlockSpec(memory_space=pltpu.VMEM)
    return pl.pallas_call(
        kernel,
        grid=(1,),
        in_specs=[block_of(spread, block)] + [whole] * (len(extra) + len(backs)),
        out_specs=whole,
        out_shape=jax.ShapeDtypeStruct((rows, backs[0].shape[1]), BF16),
        compiler_params=grant(10),
    )(spread, *extra, *backs)


def layer(
    query_heads,
    key_heads,
    value_heads,
    sink_logit,
    residual,
    out_weight,
    norm_gain,
    routes,
    route_weight,
    gate_weight,
    up_weight,
    down_weight,
):
    expert_count = lax.axis_size("sp")
    half = lax.axis_size("tp") // 2
    tok_rows = residual.shape[0]
    choose_count = routes.shape[1]
    parts = parts_of(expert_count)
    tp_index = lax.axis_index("tp")
    index = lax.axis_index("sp").astype(jnp.int32).reshape(1)

    def across(block):
        return exchange(block, "tp", lambda i: (i + half) % (2 * half))

    def to_experts(blocks):
        return [blocks[0]] + [
            exchange(blocks[d], "sp", lambda i, d=d: i ^ d)
            for d in range(1, expert_count)
        ]

    own_gate, own_up, own_down = gate_weight[0], up_weight[0], down_weight[0]
    tail = from_behind(first_moves(key_heads, value_heads), "sp")
    left, right = cut_weight(own_down)
    gates, ups, downs = [[own_gate]], [[own_up]], [[own_down]]
    own_chunks = {"gate": [own_gate], "up": [own_up], "down": [left, right]}
    for distance in range(1, half):
        for what, held in (("gate", gates), ("up", ups), ("down", downs)):
            if distance % 2:
                step, chunks = 1, held[distance - 1]
            else:
                step, chunks = distance, own_chunks[what]
            held.append([exchange(chunk, "tp", lambda i, s=step: i ^ s) for chunk in chunks])
    ups = [piece[0] for piece in ups]

    attended = attend(query_heads, key_heads, value_heads, sink_logit, tail, tok_rows)
    gathered = lax.all_to_all(attended, "tp", split_axis=0, concat_axis=0, tiled=True)

    capacity = max(2, 5 * tok_rows * choose_count // (4 * expert_count))
    slots = -(-capacity // SLOT_TILE) * SLOT_TILE
    starts = [tp_index * tok_rows, (tp_index + half) % (2 * half) * tok_rows]
    ids = jnp.stack([lax.dynamic_slice_in_dim(routes.T, at, tok_rows, 1) for at in starts])
    weight_own = route_weight.T
    weight_far = across(weight_own)
    gather = table(
        gather_kernel, (index, ids), (2, expert_count, slots, tok_rows), expert_count, slots
    )
    spread = table(
        spread_kernel,
        (index, ids, weight_own, weight_far),
        (2, expert_count, 2, tok_rows, LANES),
        expert_count,
        slots,
    )

    stream, normed, send_own = project(
        gathered, out_weight, residual, norm_gain.reshape(1, -1), gather, parts
    )
    rows_far = []
    for h in range(parts):
        far = across(normed[h])
        rows_far += to_experts(pack_far(gather, far))
    rows_own = to_experts(send_own)
    hidden_own = gate_up(rows_own, 1, gates, ups)
    hidden_far = gate_up(rows_far, parts, gates, ups)
    part_far = []
    for h in range(parts):
        backs = down(hidden_far, downs, expert_count, h, parts)
        backs = to_experts(backs)
        mixed = combine(combine_far_kernel, spread, 1, (), backs)
        part_far.append(across(mixed))
    backs = down(hidden_own, downs, expert_count, 0, 1)
    backs = to_experts(backs)
    return combine(
        functools.partial(combine_own_kernel, parts=parts), spread, 0, (stream, *part_far), backs
    )


def parts_of(expert_count):
    return 2 if expert_count <= 4 else 1


def solution(mesh):
    placed = (
        P("sp", "tp"),
        P("sp", "tp"),
        P("sp", "tp"),
        P("tp"),
        P(("sp", "tp"), None),
        P(),
        P(),
        P("sp", None),
        P(("sp", "tp"), None),
        P("sp", None, "tp"),
        P("sp", None, "tp"),
        P("sp", "tp", None),
    )
    return jax.shard_map(
        layer, mesh=mesh, in_specs=placed, out_specs=P(("sp", "tp"), None), check_vma=False
    )
```

```python
import functools

import jax
import jax.numpy as jnp
from jax import lax
from jax.experimental import pallas as pl
from jax.experimental.pallas import tpu as pltpu
from jax.sharding import PartitionSpec as P


HEAD = 64
WINDOW = 128
LANES = 128
SLOT_TILE = 16


eps = 1e-06
clamp_limit = 7.0
sigmoid_alpha = 1.702

F32 = jnp.float32
BF16 = jnp.bfloat16


def grant(mebibytes):
    return pltpu.CompilerParams(vmem_limit_bytes=mebibytes * 2**20)


def exchange(block, axis, partner):
    devices = range(lax.axis_size(axis))
    return lax.ppermute(block, axis, [(i, partner(i)) for i in devices])


def from_behind(block, axis):
    devices = range(lax.axis_size(axis))
    return lax.ppermute(block, axis, [(i - 1, i) for i in devices if i > 0])


def first_kernel(k_ref, v_ref, tail_ref):
    kv_cols = k_ref.shape[1]
    tail_ref[:, :kv_cols] = k_ref[...]
    tail_ref[:, kv_cols:] = v_ref[...]


def first_moves(key_heads, value_heads):
    span, kv_cols = key_heads.shape
    last = pl.BlockSpec((WINDOW, kv_cols), lambda i: (span // WINDOW - 1, 0))
    return pl.pallas_call(
        first_kernel,
        grid=(1,),
        in_specs=[last, last],
        out_specs=pl.BlockSpec(memory_space=pltpu.VMEM),
        out_shape=jax.ShapeDtypeStruct((WINDOW, 2 * kv_cols), BF16),
        name="first_moves",
    )(key_heads, value_heads)


def cut_kernel(down_ref, left_ref, right_ref, sems):
    cols = left_ref.shape[1]
    copies = [
        pltpu.make_async_copy(down_ref.at[:, pl.ds(0, cols)], left_ref, sems.at[0]),
        pltpu.make_async_copy(down_ref.at[:, pl.ds(cols, cols)], right_ref, sems.at[1]),
    ]
    for copy in copies:
        copy.start()
    for copy in copies:
        copy.wait()


def cut_weight(down):
    half_down = jax.ShapeDtypeStruct((down.shape[0], down.shape[1] // 2), BF16)
    return pl.pallas_call(
        cut_kernel,
        in_specs=[pl.BlockSpec(memory_space=pltpu.HBM)],
        out_specs=[pl.BlockSpec(memory_space=pltpu.VMEM)] * 2,
        out_shape=[half_down, half_down],
        scratch_shapes=[pltpu.SemaphoreType.DMA((2,))],
        name="cut_weight",
    )(down)


def attention_kernel(
    info_ref, sink_ref, q_hbm, k_hbm, v_hbm, tail_ref, out_ref, q_ref, k_ref, v_ref, kk_ref, vt_ref,
    logit_ref, spread_ref, rest_ref, sems, *, blocks, kv_local, group_size,
):
    kv_cols = kv_local * HEAD
    copies = [
        pltpu.make_async_copy(source, target, sems.at[j])
        for j, (source, target) in enumerate(((k_hbm, k_ref), (v_hbm, v_ref), (q_hbm, q_ref)))
    ]
    for copy in copies:
        copy.start()
    row = lax.broadcasted_iota(jnp.int32, (WINDOW, 2 * WINDOW), 0)
    col = lax.broadcasted_iota(jnp.int32, (WINDOW, 2 * WINDOW), 1)
    first_head = lax.broadcasted_iota(jnp.int32, (1, 2 * WINDOW), 1) < WINDOW
    before = row > lax.rem(col, WINDOW)
    low = lax.broadcasted_iota(jnp.int32, (WINDOW, 2 * HEAD), 1) < HEAD
    penalty = jnp.where(info_ref[0] == 0, -jnp.inf, 0.0)
    zeros = jnp.zeros((WINDOW, 2 * WINDOW), BF16)
    ones_rows = vt_ref.shape[1] - HEAD
    copies[0].wait()
    copies[1].wait()
    for block in range(blocks + 1):
        to = slice(block * WINDOW, (block + 1) * WINDOW)
        if block == 0:
            keys, values = tail_ref[:, :kv_cols], tail_ref[:, kv_cols:]
        else:
            at = slice((block - 1) * WINDOW, block * WINDOW)
            keys, values = k_ref[at, :], v_ref[at, :]
        turned = values.astype(F32).T.astype(BF16)
        for kv in range(kv_local):
            part = slice(kv * HEAD, (kv + 1) * HEAD)
            kk_ref[kv, to, :] = jnp.concatenate([keys[:, part], keys[:, part]], axis=1)
            vt_ref[kv, :HEAD, to] = turned[part, :]
            vt_ref[kv, HEAD:, to] = jnp.ones((ones_rows, WINDOW), BF16)
    copies[2].wait()
    per_block = out_ref.shape[0] // blocks
    pairs = kv_local * group_size // 2
    work = [(block, pair) for block in range(blocks) for pair in range(pairs)]
    for block, pair in work:
        band = slice(block * WINDOW, (block + 2) * WINDOW)
        queries = q_ref[
            block * WINDOW : (block + 1) * WINDOW, pair * 2 * HEAD : (pair + 1) * 2 * HEAD
        ] * jnp.asarray(HEAD ** (-0.5), BF16)
        blank = jnp.zeros_like(queries)
        stacked = jnp.concatenate(
            [jnp.where(low, queries, blank), jnp.where(low, blank, queries)], axis=0
        )
        scores = lax.dot_general(
            kk_ref[2 * pair // group_size, band, :],
            stacked,
            (((1,), (1,)), ((), ())),
            preferred_element_type=F32,
        )
        earlier = scores[:WINDOW, :]
        if block == 0:
            earlier = earlier + penalty
        logit_ref[block * pairs + pair] = jnp.where(before, earlier, scores[WINDOW:, :])
    for block, pair in work:
        item = block * pairs + pair
        logits = logit_ref[item]
        sink = jnp.where(first_head, sink_ref[2 * pair], sink_ref[2 * pair + 1])
        top = jnp.maximum(jnp.max(logits, axis=0, keepdims=True), sink)
        raised = jnp.exp(logits - top).astype(BF16)
        spread_ref[item, :WINDOW, :] = jnp.where(before, raised, zeros)
        spread_ref[item, WINDOW:, :] = jnp.where(before, zeros, raised)
        rest_ref[item] = jnp.broadcast_to(jnp.exp(sink - top), rest_ref.shape[1:])
    for block, pair in work:
        item = block * pairs + pair
        band = slice(block * WINDOW, (block + 2) * WINDOW)
        summed = jnp.dot(
            vt_ref[2 * pair // group_size, :, band], spread_ref[item], preferred_element_type=F32
        )
        total = summed[HEAD : HEAD + 1, :] + rest_ref[item][:1, :]
        scaled = summed[:HEAD, :] * (1.0 / total)
        turned = jnp.concatenate([scaled[:, :WINDOW], scaled[:, WINDOW:]], axis=0).T
        out_ref[
            block * per_block : (block + 1) * per_block, :, pair * 2 * HEAD : (pair + 1) * 2 * HEAD
        ] = turned.astype(BF16).reshape((per_block, out_ref.shape[1], 2 * HEAD))


def attend(query_heads, key_heads, value_heads, sink_logit, tail, tok_rows):
    span, q_cols = query_heads.shape
    kv_cols = key_heads.shape[1]
    kv_local = kv_cols // HEAD
    smem = pl.BlockSpec(memory_space=pltpu.SMEM)
    whole = pl.BlockSpec(memory_space=pltpu.VMEM)
    stored = pl.BlockSpec(memory_space=pltpu.HBM)
    items = span // WINDOW * q_cols // (2 * HEAD)
    info = lax.axis_index("sp").astype(jnp.int32).reshape(1)
    return pl.pallas_call(
        functools.partial(
            attention_kernel,
            blocks=span // WINDOW,
            kv_local=kv_local,
            group_size=q_cols // kv_cols,
        ),
        in_specs=[smem, smem] + [stored] * 3 + [whole],
        out_specs=whole,
        out_shape=jax.ShapeDtypeStruct((span // tok_rows, tok_rows, q_cols), BF16),
        scratch_shapes=[
            pltpu.VMEM((span, q_cols), BF16),
            pltpu.VMEM((span, kv_cols), BF16),
            pltpu.VMEM((span, kv_cols), BF16),
            pltpu.VMEM((kv_local, span + WINDOW, 2 * HEAD), BF16),
            pltpu.VMEM((kv_local, HEAD + SLOT_TILE, span + WINDOW), BF16),
            pltpu.VMEM((items, WINDOW, 2 * WINDOW), F32),
            pltpu.VMEM((items, 2 * WINDOW, 2 * WINDOW), BF16),
            pltpu.VMEM((items, 8, 2 * WINDOW), F32),
            pltpu.SemaphoreType.DMA((3,)),
        ],
        name="attend",
    )(info, sink_logit, query_heads, key_heads, value_heads, tail)


def slots_of(ids, expert, slots):
    choices, rows = ids.shape
    chosen = jnp.zeros((8, rows), F32)
    for k in range(choices):
        match = jnp.broadcast_to(ids[k : k + 1, :], (8, rows)) == expert
        chosen += jnp.where(match, 1.0, 0.0)
    earlier = lax.broadcasted_iota(jnp.int32, (rows, rows), 0) < lax.broadcasted_iota(
        jnp.int32, (rows, rows), 1
    )
    rank = jnp.dot(
        chosen.astype(BF16), earlier.astype(F32).astype(BF16), preferred_element_type=F32
    )
    place = jnp.where(chosen > 0.5, rank, -1.0).astype(jnp.int32)
    return lax.broadcasted_iota(jnp.int32, (slots, rows), 0) == place[:1, :]


def gather_kernel(info_ref, ids_ref, gather_ref, *, expert_count, slots):
    for block in range(ids_ref.shape[0]):
        for distance in range(expert_count):
            hot = slots_of(ids_ref[block], info_ref[0] ^ distance, slots)
            gather_ref[block, distance] = hot.astype(F32).astype(BF16)


def spread_kernel(info_ref, ids_ref, *refs, expert_count, slots):
    weight_refs, spread_ref = refs[:-1], refs[-1]
    blocks, choices, rows = ids_ref.shape
    for block in range(blocks):
        ids = ids_ref[block]
        for distance in range(expert_count):
            expert = info_ref[0] ^ distance
            weight = jnp.zeros((1, rows), F32)
            for k in range(choices):
                match = ids[k : k + 1, :] == expert
                weight += jnp.where(match, weight_refs[block][k : k + 1, :], 0.0)
            weight = jnp.where(slots_of(ids, expert, LANES), weight, 0.0).T
            high = weight.astype(BF16)
            spread_ref[block, distance, 0] = high
            spread_ref[block, distance, 1] = (weight - high.astype(F32)).astype(BF16)


def table(kernel, operands, shape, expert_count, slots):
    whole = pl.BlockSpec(memory_space=pltpu.VMEM)
    return pl.pallas_call(
        functools.partial(kernel, expert_count=expert_count, slots=slots),
        in_specs=[pl.BlockSpec(memory_space=pltpu.SMEM)] + [whole] * (len(operands) - 1),
        out_specs=whole,
        out_shape=jax.ShapeDtypeStruct(shape, BF16),
        compiler_params=grant(4),
    )(*operands)


def project_kernel(att_ref, w_hbm, res_ref, gain_ref, stream_ref, *refs, parts, tile):
    part_refs = refs[:parts]
    acc_ref, w_ref, sems = refs[parts:]
    sources, _, cols = att_ref.shape
    width = stream_ref.shape[1]
    copies = []
    for n in range(width // tile):
        part = pl.ds(n * tile, tile)
        copies.append(pltpu.make_async_copy(w_hbm.at[:, part], w_ref.at[n], sems.at[n]))
    for copy in copies:
        copy.start()
    square = None
    for n in range(width // tile):
        part = slice(n * tile, (n + 1) * tile)
        copies[n].wait()
        total = None
        for k in range(sources):
            piece = jnp.dot(
                att_ref[k], w_ref[n, k * cols : (k + 1) * cols, :], preferred_element_type=F32
            )
            total = piece if total is None else total + piece
        stream = (res_ref[:, part].astype(F32) + total).astype(BF16)
        stream_ref[:, part] = stream
        wide = stream.astype(F32)
        acc_ref[:, part] = wide
        summed = jnp.sum(wide * wide, axis=-1, keepdims=True)
        square = summed if square is None else square + summed
    scale = lax.rsqrt(square / width + eps)
    step = width // parts
    for h in range(parts):
        part = slice(h * step, (h + 1) * step)
        part_refs[h][...] = (acc_ref[:, part] * scale * gain_ref[:, part]).astype(BF16)


def project(gathered, out_weight, residual, norm_gain, parts):
    _, rows, _ = gathered.shape
    width = out_weight.shape[1]
    tile = min(512, width)
    whole = pl.BlockSpec(memory_space=pltpu.VMEM)
    outs = pl.pallas_call(
        functools.partial(project_kernel, parts=parts, tile=tile),
        in_specs=[whole, pl.BlockSpec(memory_space=pltpu.HBM), whole, whole],
        out_specs=[whole] * (1 + parts),
        out_shape=[jax.ShapeDtypeStruct((rows, width), BF16)]
        + [jax.ShapeDtypeStruct((rows, width // parts), BF16)] * parts,
        scratch_shapes=[
            pltpu.VMEM((rows, width), F32),
            pltpu.VMEM((width // tile, out_weight.shape[0], tile), BF16),
            pltpu.SemaphoreType.DMA((width // tile,)),
        ],
        name="project",
    )(gathered, out_weight, residual, norm_gain)
    return outs[0], outs[1:]


def pack_kernel(gather_ref, *refs, parts):
    part_refs, send_refs = refs[:parts], refs[parts:]
    step = part_refs[0].shape[1]
    for distance, send_ref in enumerate(send_refs):
        for h in range(parts):
            send_ref[:, h * step : (h + 1) * step] = jnp.dot(
                gather_ref[0, distance], part_refs[h][...], preferred_element_type=F32
            ).astype(BF16)


def block_of(array, block):
    zeros = (0,) * (array.ndim - 1)
    return pl.BlockSpec((1,) + array.shape[1:], lambda i: (block,) + zeros)


def pack(gather, block, rows):
    _, expert_count, slots, _ = gather.shape
    width = sum(part.shape[1] for part in rows)
    whole = pl.BlockSpec(memory_space=pltpu.VMEM)
    return pl.pallas_call(
        functools.partial(pack_kernel, parts=len(rows)),
        grid=(1,),
        in_specs=[block_of(gather, block)] + [whole] * len(rows),
        out_specs=[whole] * expert_count,
        out_shape=[jax.ShapeDtypeStruct((slots, width), BF16)] * expert_count,
        compiler_params=grant(6),
        name="pack",
    )(gather, *rows)


def gate_up_kernel(*refs, groups, parts, slots, pieces, hid, chunks):
    row_refs, refs = refs[: groups * parts], refs[groups * parts :]
    count = sum(chunks)
    gate_refs, ups = refs[:count], refs[count : count + pieces]
    hidden_ref, picked_ref, weight_ref, sems = refs[count + pieces :]
    copies, at = [], 0
    for p in range(pieces):
        group, row = [], 0
        for chunk in gate_refs[at : at + chunks[p]]:
            target = weight_ref.at[p, 0, pl.ds(row, chunk.shape[0])]
            group.append(pltpu.make_async_copy(chunk, target, sems.at[p, len(group)]))
            row += chunk.shape[0]
        at += chunks[p]
        group.append(pltpu.make_async_copy(ups[p], weight_ref.at[p, 1], sems.at[p, len(group)]))
        copies.append(group)
    for group in copies:
        for copy in group:
            copy.start()
    step = picked_ref.shape[1] // parts
    for b in range(groups):
        for h in range(parts):
            rows = row_refs[h * groups + b][...]
            picked_ref[b * slots : (b + 1) * slots, h * step : (h + 1) * step] = rows
    picked = picked_ref[...]
    for p in range(pieces):
        for copy in copies[p]:
            copy.wait()
        gate_pre = jnp.dot(picked, weight_ref[p, 0], preferred_element_type=F32)
        upward = jnp.dot(picked, weight_ref[p, 1], preferred_element_type=F32)
        capped = jnp.minimum(gate_pre, clamp_limit)
        linear = jnp.clip(upward, -clamp_limit, clamp_limit)
        hidden = capped * jax.nn.sigmoid(sigmoid_alpha * capped) * (linear + 1.0)
        hidden_ref[:, p * hid : (p + 1) * hid] = hidden.astype(BF16)


def gate_up(rows, parts, gates, ups):
    groups, pieces = len(rows) // parts, len(gates)
    slots = rows[0].shape[0]
    width, hid = ups[0].shape
    chunks = tuple(len(piece) for piece in gates)
    flat = [chunk for piece in gates for chunk in piece]
    whole = pl.BlockSpec(memory_space=pltpu.VMEM)
    stored = pl.BlockSpec(memory_space=pltpu.HBM)
    return pl.pallas_call(
        functools.partial(
            gate_up_kernel,
            groups=groups,
            parts=parts,
            slots=slots,
            pieces=pieces,
            hid=hid,
            chunks=chunks,
        ),
        in_specs=[whole] * len(rows) + [stored] * (len(flat) + pieces),
        out_specs=whole,
        out_shape=jax.ShapeDtypeStruct((groups * slots, pieces * hid), BF16),
        scratch_shapes=[
            pltpu.VMEM((groups * slots, width), BF16),
            pltpu.VMEM((pieces, 2, width, hid), BF16),
            pltpu.SemaphoreType.DMA((pieces, max(chunks) + 1)),
        ],
        compiler_params=grant(20),
    )(*rows, *flat, *ups)


def down_kernel(hidden_ref, *refs, groups, slots, hid, chunks, tile):
    out_refs = refs[sum(chunks) :]
    width = out_refs[0].shape[1]
    for n in range(width // tile):
        total, at = None, 0
        for p, count in enumerate(chunks):
            ref = refs[at + n * tile * count // width]
            start = n * tile % (width // count)
            at += count
            part = jnp.dot(
                hidden_ref[:, p * hid : (p + 1) * hid],
                ref[:, start : start + tile],
                preferred_element_type=F32,
            )
            total = part if total is None else total + part
        expert_out = total.astype(BF16)
        for b in range(groups):
            out_refs[b][:, n * tile : (n + 1) * tile] = expert_out[b * slots : (b + 1) * slots, :]


def down(hidden, downs, groups, part, parts):
    hid = downs[0][0].shape[0]
    full = sum(chunk.shape[1] for chunk in downs[0])
    width = full // parts
    slots = hidden.shape[0] // groups
    whole = pl.BlockSpec(memory_space=pltpu.VMEM)
    operands, specs, chunks = [], [], []
    for piece in downs:
        if len(piece) == 1:
            operands.append(piece[0])
            specs.append(pl.BlockSpec((hid, width), lambda i: (0, part)))
            chunks.append(1)
        else:
            used = piece[part * len(piece) // parts : (part + 1) * len(piece) // parts]
            operands += used
            specs += [whole] * len(used)
            chunks.append(len(used))
    body = functools.partial(
        down_kernel,
        groups=groups,
        slots=slots,
        hid=hid,
        chunks=tuple(chunks),
        tile=min(512, width),
    )
    return pl.pallas_call(
        body,
        grid=(1,),
        in_specs=[whole] + specs,
        out_specs=[whole] * groups,
        out_shape=[jax.ShapeDtypeStruct((slots, width), BF16)] * groups,
        compiler_params=grant(12),
    )(hidden, *operands)


def unpack(spread_ref, back_refs):
    slots = back_refs[0].shape[0]
    total = None
    for term in (1, 0):
        for distance, back_ref in enumerate(back_refs):
            part = jnp.dot(
                spread_ref[0, distance, term][:, :slots], back_ref[...], preferred_element_type=F32
            )
            total = part if total is None else total + part
    return total


def combine_far_kernel(spread_ref, *refs):
    refs[-1][...] = unpack(spread_ref, refs[:-1]).astype(BF16)


def combine_own_kernel(spread_ref, stream_ref, *refs):
    refs[-1][...] = unpack(spread_ref, refs[:-1]) + stream_ref[...].astype(F32)


def finish_kernel(own_ref, *refs):
    out_ref = refs[-1]
    step = refs[0].shape[1]
    for h, far_ref in enumerate(refs[:-1]):
        cols = slice(h * step, (h + 1) * step)
        out_ref[:, cols] = (own_ref[:, cols] + far_ref[...].astype(F32)).astype(BF16)


def finish(own, parts):
    whole = pl.BlockSpec(memory_space=pltpu.VMEM)
    return pl.pallas_call(
        finish_kernel,
        in_specs=[whole] * (1 + len(parts)),
        out_specs=whole,
        out_shape=jax.ShapeDtypeStruct(own.shape, BF16),
        compiler_params=grant(10),
        name="finish",
    )(own, *parts)


def combine(kernel, spread, block, extra, backs, dtype):
    rows = spread.shape[3]
    whole = pl.BlockSpec(memory_space=pltpu.VMEM)
    return pl.pallas_call(
        kernel,
        grid=(1,),
        in_specs=[block_of(spread, block)] + [whole] * (len(extra) + len(backs)),
        out_specs=whole,
        out_shape=jax.ShapeDtypeStruct((rows, backs[0].shape[1]), dtype),
        compiler_params=grant(10),
    )(spread, *extra, *backs)


def layer(
    query_heads,
    key_heads,
    value_heads,
    sink_logit,
    residual,
    out_weight,
    norm_gain,
    routes,
    route_weight,
    gate_weight,
    up_weight,
    down_weight,
):
    expert_count = lax.axis_size("sp")
    half = lax.axis_size("tp") // 2
    tok_rows = residual.shape[0]
    choose_count = routes.shape[1]
    parts = parts_of(expert_count)
    tp_index = lax.axis_index("tp")
    index = lax.axis_index("sp").astype(jnp.int32).reshape(1)

    def across(block):
        return exchange(block, "tp", lambda i: (i + half) % (2 * half))

    def to_experts(blocks):
        return [blocks[0]] + [
            exchange(blocks[d], "sp", lambda i, d=d: i ^ d)
            for d in range(1, expert_count)
        ]

    own_gate, own_up, own_down = gate_weight[0], up_weight[0], down_weight[0]
    tail = from_behind(first_moves(key_heads, value_heads), "sp")
    left, right = cut_weight(own_down)
    gates, ups, downs = [[own_gate]], [[own_up]], [[own_down]]
    own_chunks = {"gate": [own_gate], "up": [own_up], "down": [left, right]}
    for distance in range(1, half):
        for what, held in (("gate", gates), ("up", ups), ("down", downs)):
            if distance % 2:
                step, chunks = 1, held[distance - 1]
            else:
                step, chunks = distance, own_chunks[what]
            held.append([exchange(chunk, "tp", lambda i, s=step: i ^ s) for chunk in chunks])
    ups = [piece[0] for piece in ups]

    attended = attend(query_heads, key_heads, value_heads, sink_logit, tail, tok_rows)
    gathered = lax.all_to_all(attended, "tp", split_axis=0, concat_axis=0, tiled=True)

    capacity = max(2, 5 * tok_rows * choose_count // (4 * expert_count))
    slots = -(-capacity // SLOT_TILE) * SLOT_TILE
    starts = [tp_index * tok_rows, (tp_index + half) % (2 * half) * tok_rows]
    ids = jnp.stack([lax.dynamic_slice_in_dim(routes.T, at, tok_rows, 1) for at in starts])
    weight_own = route_weight.T
    weight_far = across(weight_own)
    gather = table(
        gather_kernel, (index, ids), (2, expert_count, slots, tok_rows), expert_count, slots
    )
    spread = table(
        spread_kernel,
        (index, ids, weight_own, weight_far),
        (2, expert_count, 2, tok_rows, LANES),
        expert_count,
        slots,
    )

    stream, normed = project(gathered, out_weight, residual, norm_gain.reshape(1, -1), parts)
    rows_far = []
    for h in range(parts):
        far = across(normed[h])
        rows_far += to_experts(pack(gather, 1, (far,)))
    rows_own = to_experts(pack(gather, 0, normed))
    hidden_own = gate_up(rows_own, 1, gates, ups)
    hidden_far = gate_up(rows_far, parts, gates, ups)
    part_far = []
    for h in range(parts):
        backs = down(hidden_far, downs, expert_count, h, parts)
        backs = to_experts(backs)
        mixed = combine(combine_far_kernel, spread, 1, (), backs, BF16)
        part_far.append(across(mixed))
    backs = down(hidden_own, downs, expert_count, 0, 1)
    backs = to_experts(backs)
    own = combine(combine_own_kernel, spread, 0, (stream,), backs, F32)
    return finish(own, part_far)


def parts_of(expert_count):
    return 2 if expert_count <= 4 else 1


def solution(mesh):
    placed = (
        P("sp", "tp"),
        P("sp", "tp"),
        P("sp", "tp"),
        P("tp"),
        P(("sp", "tp"), None),
        P(),
        P(),
        P("sp", None),
        P(("sp", "tp"), None),
        P("sp", None, "tp"),
        P("sp", None, "tp"),
        P("sp", "tp", None),
    )
    return jax.shard_map(
        layer, mesh=mesh, in_specs=placed, out_specs=P(("sp", "tp"), None), check_vma=False
    )
```
